32 devices in a mesh: sp: 8 (over z, x), tp: 4 (over y, core).
Axes of the slice: x: 2, y: 2, z: 4, core: 2. Of those that a mesh axis runs over, the one named last changes fastest.
Arguments:
- stream_in: bfloat16 [2048, 2048], P(('sp', 'tp')), may hold values from -6 to 6
- pre_gate: bfloat16 [2048, 1024], P('sp', 'tp'), may hold values from -6 to 6
- value_in: bfloat16 [2048, 1024], P('sp', 'tp'), may hold values from -6 to 6
- post_gate: bfloat16 [2048, 1024], P('sp', 'tp'), may hold values from -6 to 6
- conv_taps: bfloat16 [3, 1024], P(None, 'tp'), may hold values from -3 to 3
- out_weight: bfloat16 [1024, 2048], P('tp'), may hold values from -0.1875 to 0.1875
- route_ids: int32 [2048, 4], P('sp'), may hold values from 0 to 7, all different within a row; in each aligned block of 64 rows (0 to 63, 64 to 127, ...) at most 64 rows name the same one
- route_weight: float32 [2048, 4], P('sp'), may hold values from 0.1 to 1
- ffn_gain: bfloat16 [2048], replicated, may hold values from 0.099609375 to 1.8984375
- post_gain: bfloat16 [2048], replicated, may hold values from 0.099609375 to 1.8984375
- gate_proj: bfloat16 [8, 2048, 2048], P('sp', None, 'tp'), may hold values from -0.39648438 to 0.39648438
- up_proj: bfloat16 [8, 2048, 2048], P('sp', None, 'tp'), may hold values from -0.39648438 to 0.39648438
- down_proj: bfloat16 [8, 2048, 2048], P('sp', None, 'tp'), may hold values from -0.125 to 0.125
Outputs:
- layer_out: bfloat16 [2048, 2048], P(('sp', 'tp'))
The draws below stay inside these ranges and needn't reach their ends.
Inputs may be any that keep to these rules, and one draw needn't show every extreme that they name: `route_ids`: in each aligned block of 64 positions, a row names 4 different experts and no expert is named by more than 64 rows; in every draw some expert reaches 64 in some block.
All inputs are finite; a program needn't handle non-finite values.
Results may differ from the reference program's by a relative error of at most 0.014.
Values may be sent and summed in bfloat16 or wider, within the bound.
A program may use at most 64 MiB of HBM per device.

```python
import math
import jax
import jax.numpy as jnp
import numpy as np
from jax import lax

D = 2048
W = 1024
FF = 2048
TOPK = 4
KERNEL = 3
TOKENS = 2048
EXPERTS = 8
ROWS = 64
CAP = 64
SLOTS = 2048


def shard_levels(key, extent, shards, low, top_value):
    level, own = 1.0, jax.random.fold_in(key, 6)
    for position, blocks in shards:
        heights = jnp.exp(jax.random.uniform(jax.random.fold_in(own, position), (blocks,), jnp.float32, low / len(shards), top_value / len(shards)))
        level = level * jnp.repeat(heights, extent[position] // blocks).reshape([-1 if axis == position else 1 for axis in range(len(extent))])
    return level


def deal_out(stream_key, own, number, rows, count, top, bound, slope):
    sequence = jax.random.permutation(stream_key, count)
    crowded, ordinary = load_shares(count, rows * top, bound, slope, True), load_shares(count, rows * top, bound, slope, False)
    places = jnp.arange(count)

    def named(lengths, rotation):
        used = int((lengths > 0).sum())
        fixed = max(1, used // 4)
        moved = fixed + (places - fixed + rotation * (used - fixed)) % max(1, count - fixed)
        return jnp.zeros((count,), jnp.int32).at[sequence[jnp.where(places < fixed, places, moved)]].set(jnp.asarray(lengths, jnp.int32))

    lengths = jnp.where(number % 4 == 0, named(crowded, number // 4), named(ordinary, number - number // 4 - 1))
    mixed = jax.random.permutation(jax.random.fold_in(own, 3), count)
    donor, receiver = mixed[0:count // 2 * 2:2], mixed[1:count // 2 * 2:2]
    margin = jnp.minimum(lengths[donor] - 1, bound - lengths[receiver]) // 2
    margin = jnp.where((donor == sequence[0]) | (receiver == sequence[0]) | (lengths[receiver] == 0), 0, jnp.maximum(margin, 0))
    moved = jax.random.randint(jax.random.fold_in(own, 4), (count // 2,), 0, 1 << 20) % (margin + 1)
    lengths = lengths.at[donor].add(-moved).at[receiver].add(moved)
    members = jnp.searchsorted(jnp.cumsum(lengths), jnp.arange(rows * top), side="right").astype(jnp.int32)
    grid = members.reshape(top, rows).T
    grid = grid[jax.random.permutation(jax.random.fold_in(own, 1), rows)]
    rotation = jax.random.randint(jax.random.fold_in(own, 2), (rows, 1), 0, top)
    return jnp.take_along_axis(grid, (jnp.arange(top)[None, :] + rotation) % top, axis=1)


def load_shares(number_of, total, bound, lean, full):
    portions = [(1 << 20) // math.isqrt(standing ** lean) + 1 for standing in range(1, number_of + 1)]
    largest = bound if full else min(bound, max(-(-total // number_of), total * portions[0] // sum(portions)))
    least = 1 if total - largest >= number_of - 1 else 0
    counts, rest = [largest] + [least] * (number_of - 1), total - largest - least * (number_of - 1)
    while rest > 0:
        candidates = [i for i in range(1, number_of) if counts[i] < largest] or [i for i in range(1, number_of) if counts[i] < bound]
        whole, remaining = sum([portions[i] for i in candidates]), rest
        for i in candidates:
            addition = min(bound - counts[i], max(1, remaining * portions[i] // whole), rest)
            counts[i] = counts[i] + addition
            rest = rest - addition
    return np.array(counts)


def normal_values(rng, extent, width, limit, split=(), kind=jnp.bfloat16):
    drawn = width * jax.random.normal(rng, extent, jnp.float32)
    if split:
        drawn = drawn * shard_levels(rng, extent, split, -0.22, 0.18)
    return jnp.clip(drawn, -limit, limit).astype(kind)


def setup_inputs(seed: int = 0) -> dict:
    key_of = jax.random.split(jax.random.key(seed), 14)
    stream_in = normal_values(key_of[0], (TOKENS, D), 1.0, 6.0, ((0, 32),))
    pre_gate = normal_values(key_of[1], (TOKENS, W), 1.0, 6.0, ((0, 8), (1, 4)))
    value_in = normal_values(key_of[2], (TOKENS, W), 1.0, 6.0, ((0, 8), (1, 4)))
    post_gate = normal_values(key_of[3], (TOKENS, W), 1.0, 6.0, ((0, 8), (1, 4)))
    conv_taps = normal_values(key_of[4], (KERNEL, W), 0.6, 3.0, ((1, 4),))
    out_weight = normal_values(key_of[5], (W, D), W ** -0.5, 0.1875, ((0, 4),))
    route_ids_keys = jax.random.split(jax.random.fold_in(key_of[6], 1), TOKENS // ROWS)
    route_ids_turns = jax.random.permutation(jax.random.fold_in(key_of[6], 3), TOKENS // ROWS)
    route_ids = jax.vmap(lambda own, number: deal_out(jax.random.fold_in(key_of[6], 2), own, number, ROWS, EXPERTS, TOPK, CAP, 2))(route_ids_keys, route_ids_turns).reshape((TOKENS, TOPK))
    route_weight = jnp.clip(jnp.exp(math.log(1.0) - 2.3025851 * jax.random.uniform(key_of[7], (TOKENS, TOPK), jnp.float32) ** shard_levels(key_of[7], (TOKENS, TOPK), ((0, 8),), -0.2, 0.2)), 0.1, 1.0)
    ffn_gain = jnp.clip(1.0 + 0.18 * jax.random.normal(key_of[8], (D,), jnp.float32), 0.099609375, 1.8984375).astype(jnp.bfloat16)
    post_gain = jnp.clip(1.0 + 0.18 * jax.random.normal(key_of[9], (D,), jnp.float32), 0.099609375, 1.8984375).astype(jnp.bfloat16)
    gate_proj = normal_values(key_of[10], (EXPERTS, D, FF), (3.0 * D ** -0.5), 0.39648438, ((0, 8), (2, 4)))
    up_proj = normal_values(key_of[11], (EXPERTS, D, FF), (3.0 * D ** -0.5), 0.39648438, ((0, 8), (2, 4)))
    down_proj = normal_values(key_of[12], (EXPERTS, FF, D), FF ** -0.5, 0.125, ((0, 8), (2, 4)))
    return dict(stream_in=stream_in, pre_gate=pre_gate, value_in=value_in, post_gate=post_gate, conv_taps=conv_taps, out_weight=out_weight, route_ids=route_ids, route_weight=route_weight, ffn_gain=ffn_gain, post_gain=post_gain, gate_proj=gate_proj, up_proj=up_proj, down_proj=down_proj)


clamp_limit = 7.0
sigmoid_scale = 1.702
epsilon = 1e-06

def clamped_units(gate_pre, up_pre):
    gate_cut = jnp.minimum(gate_pre, clamp_limit)
    up_cut = jnp.clip(up_pre, -clamp_limit, clamp_limit)
    return (up_cut + 1.0) * (gate_cut * jax.nn.sigmoid(sigmoid_scale * gate_cut))

def scaled_norm(values, gain):
    return values * lax.rsqrt(lax.optimization_barrier(jnp.mean(values * values, axis=-1, keepdims=True)) + epsilon) * gain.astype(jnp.float32)

def reference(stream_in, pre_gate, value_in, post_gate, conv_taps, out_weight, route_ids, route_weight, ffn_gain, post_gain, gate_proj, up_proj, down_proj):
    tap_count = conv_taps.shape[0]
    gated_input = (pre_gate.astype(jnp.float32) * value_in.astype(jnp.float32)).astype(jnp.bfloat16)
    padded = jnp.concatenate([jnp.zeros((tap_count - 1, W), jnp.bfloat16), gated_input], 0).astype(jnp.float32)
    convolved = jnp.zeros((TOKENS, W), jnp.float32)
    for tap_index in range(tap_count):
        convolved = convolved + conv_taps[tap_index].astype(jnp.float32)[None, :] * padded[tap_index:tap_index + TOKENS]
    mixer_out = (post_gate.astype(jnp.float32) * convolved).astype(jnp.bfloat16)
    projected = jnp.dot(mixer_out, out_weight, preferred_element_type=jnp.float32)
    residual = (stream_in.astype(jnp.float32) + projected).astype(jnp.bfloat16)
    normed = scaled_norm(residual.astype(jnp.float32), ffn_gain).astype(jnp.bfloat16)
    flattened = route_ids.reshape(-1).astype(jnp.int32)
    entries = flattened.shape[0]
    onehot = (flattened[:, None] == jnp.arange(EXPERTS, dtype=jnp.int32)[None, :]).astype(jnp.int32)
    blocked = onehot.reshape(entries // (ROWS * TOPK), ROWS * TOPK, EXPERTS)
    before = jnp.cumsum(blocked, axis=1) - blocked
    slot_rank = lax.optimization_barrier(jnp.sum(before * blocked, axis=2)).reshape(entries)
    block_ids = jnp.arange(entries, dtype=jnp.int32) // (ROWS * TOPK)
    slot_index = (block_ids * CAP + slot_rank).astype(jnp.int32)
    token_ids = jnp.arange(entries, dtype=jnp.int32) // TOPK
    slot_table = jnp.full((EXPERTS, SLOTS), TOKENS, jnp.int32).at[flattened, slot_index].set(token_ids)
    padded_rows = jnp.concatenate([normed, jnp.zeros((1, D), jnp.bfloat16)], 0)

    def one_expert(packed):
        token_rows, gate_matrix, up_matrix, down_matrix = packed
        inputs = padded_rows[token_rows]
        gate_pre = jnp.dot(inputs, gate_matrix, preferred_element_type=jnp.float32)
        up_pre = jnp.dot(inputs, up_matrix, preferred_element_type=jnp.float32)
        hidden = clamped_units(gate_pre, up_pre).astype(jnp.bfloat16)
        return jnp.dot(hidden, down_matrix, preferred_element_type=jnp.float32).astype(jnp.bfloat16)
    expert_outs = lax.map(one_expert, (slot_table, gate_proj, up_proj, down_proj))
    picked = expert_outs[flattened, slot_index].astype(jnp.float32).reshape(TOKENS, TOPK, D)
    combined = lax.optimization_barrier(jnp.sum(picked * route_weight[:, :, None], axis=1)).astype(jnp.bfloat16)
    layer_out = residual.astype(jnp.float32) + scaled_norm(combined.astype(jnp.float32), post_gain)
    return layer_out.astype(jnp.bfloat16)
```

```python
import functools

import jax
import jax.numpy as jnp
from jax import lax
from jax.experimental import pallas as pl
from jax.experimental.pallas import tpu as pltpu
from jax.sharding import PartitionSpec as P

clamp_limit = 7.0
sigmoid_scale = 1.702
epsilon = 1e-06


def passed_along(array, axis, by):
    count = lax.axis_size(axis)
    pairs = [(i, i + by) for i in range(count) if 0 <= i + by < count]
    return lax.ppermute(array, axis, pairs)


def clamped_units(gate_pre, up_pre):
    gate_cut = jnp.minimum(gate_pre, clamp_limit)
    up_cut = jnp.clip(up_pre, -clamp_limit, clamp_limit)
    return (up_cut + 1.0) * (gate_cut * jax.nn.sigmoid(sigmoid_scale * gate_cut))


def scaled_norm(values, gain):
    return (
        values
        * lax.rsqrt(jnp.mean(values * values, axis=-1, keepdims=True) + epsilon)
        * gain.astype(jnp.float32)
    )


def block_ranks(route_rows, experts, block_rows):
    flattened = route_rows.reshape(-1)
    entries = flattened.shape[0]
    span_width = block_rows * route_rows.shape[1]
    onehot = (flattened[:, None] == jnp.arange(experts, dtype=jnp.int32)[None, :]).astype(jnp.int32)
    blocked = onehot.reshape(entries // span_width, span_width, experts)
    before = jnp.cumsum(blocked, axis=1) - blocked
    return jnp.sum(before * blocked, axis=2).reshape(route_rows.shape)


def slot_picker(slot_index, table_size):
    matches = slot_index[None, :, :] == jnp.arange(table_size, dtype=jnp.int32)[:, None, None]
    return jnp.any(matches, axis=2).astype(jnp.bfloat16)


PIECES = 4
PLANNED_GROUPS = 8
end_plan = (
    32, 33, 4, 8, 10, 5, 96, 11, 35, 6, 16, 7, 34, 18, 98, 19, 43, 9, 17, 97,
    104, 26, 24, 48, 25, 27, 51, 49, 42, 41, 40, 50, 131, 108, 31, 28, 106, 30, 29, 66,
    58, 57, 64, 109, 56, 59, 137, 141, 110, 173, 60, 63, 62, 67, 61, 65, 140, 111, 172, 22,
    38, 23, 102, 143, 129, 39, 21, 20, 36, 15, 175, 142, 105, 55, 37, 174, 13, 12, 99, 53,
    54, 52, 139, 135, 14, 169, 107, 128, 136, 101, 171, 161, 130, 44, 168, 47, 45, 163, 46, 138,
    103, 170, 100, 160, 167, 162, 134, 132, 166, 194, 133, 164, 165, 195, 192, 193,
)
middle_plan = (
    9, 8, 16, 18, 96, 19, 10, 17, 4, 34, 104, 24, 11, 26, 5, 6, 7, 12, 14, 15,
    13, 25, 27, 100, 28, 108, 101, 31, 49, 51, 50, 48, 30, 29, 71, 109, 106, 68, 69, 97,
    33, 70, 58, 47, 46, 141, 140, 44, 45, 23, 32, 22, 20, 21, 103, 137, 133, 59, 56, 105,
    172, 57, 35, 165, 173, 60, 62, 63, 61, 40, 41, 111, 110, 136, 139, 42, 55, 43, 204, 129,
    205, 132, 52, 54, 169, 65, 66, 64, 67, 142, 53, 102, 168, 174, 128, 134, 107, 143, 206, 166,
    38, 197, 175, 135, 207, 171, 98, 167, 198, 37, 39, 36, 160, 138, 203, 161, 99, 199, 164, 170,
    196, 202, 131, 163, 195, 130, 201, 162, 200, 194, 192, 193,
)

def words_of(plan):
    codes = list(plan)
    codes += [255] * (-len(codes) % 4)
    words = [sum(code << (8 * i) for i, code in enumerate(codes[at : at + 4])) for at in range(0, len(codes), 4)]
    return [word - (1 << 32) if word >> 31 else word for word in words]


def pick(at_end, tables, position):
    value = jnp.int32(-1)
    for i, table in enumerate(tables):
        chosen = jnp.int32(-1)
        for j, word in enumerate(table):
            chosen = jnp.where(position == j, word, chosen)
        value = jnp.where(at_end == (i == 0), chosen, value)
    return value


def layer_kernel(
    sp_count,
    stream_ref,
    pre_ref,
    value_ref,
    post_ref,
    taps_ref,
    ids_ref,
    weight_ref,
    gain_ref,
    post_gain_ref,
    out_hbm,
    gate_hbm,
    up_hbm,
    down_hbm,
    result_ref,
    out_w,
    gate_w,
    up_w,
    down_w,
    tail,
    rim,
    padded,
    mixed,
    pair_send,
    pair_in,
    own_sum,
    y_send,
    y_in,
    resid,
    scales,
    tokens,
    hidden,
    part,
    chain_in,
    x_in,
    total,
    final,
    columns,
    load_sem,
    rim_sem,
    pair_sem,
    y_sem,
    y_recv,
    scale_send,
    scale_recv,
    tok_send,
    tok_recv,
    mate_recv,
    hid_send,
    hid_recv,
    chain_send,
    chain_recv,
    x_send,
    x_recv,
    fin_send,
    fin_recv,
):
    f32, bf16 = jnp.float32, jnp.bfloat16
    heights = sp_count // 2
    last = heights - 1
    sp = lax.axis_index("sp")
    tp = lax.axis_index("tp")
    z, x = lax.div(sp, 2), lax.rem(sp, 2)
    y, c = lax.div(tp, 2), lax.rem(tp, 2)
    across, sibling = sp + 1 - 2 * x, tp + 1 - 2 * c
    opposite = lax.rem(tp + 2, 4)
    rows, width = stream_ref.shape
    seq = 4 * rows
    half = 2 * rows
    step = rows // PIECES
    units = gate_w.shape[1]
    at_end = (z == 0) | (z == last)
    toward = jnp.where(2 * z < heights, 1, -1)

    def at(sp_to, tp_to):
        return {"sp": sp_to, "tp": tp_to}

    def remote(source, target, send, receive, device):
        return pltpu.make_async_remote_copy(
            src_ref=source,
            dst_ref=target,
            send_sem=send,
            recv_sem=receive,
            device_id=device,
            device_id_type=pl.DeviceIdType.MESH,
        )

    loads = [
        pltpu.make_async_copy(source, target, load_sem.at[i])
        for i, (source, target) in enumerate(
            ((out_hbm, out_w), (gate_hbm.at[0], gate_w), (up_hbm.at[0], up_w), (down_hbm.at[0], down_w))
        )
    ]
    for load in loads:
        load.start()

    barrier = pltpu.get_barrier_semaphore()

    def greet(partner):
        pl.semaphore_signal(barrier, inc=1, device_id=partner, device_id_type=pl.DeviceIdType.MESH)

    for partner in (at(across, tp), at(sp, sibling), at(sp, opposite), at(sp, 3 - tp)):
        greet(partner)
    met = jnp.int32(4)
    for there, by in ((sp < sp_count - 1, 1), (sp > 0, -1), (z < last, 2), (z > 0, -2)):

        @pl.when(there)
        def _():
            greet(at(sp + by, tp))

        met = met + jnp.where(there, 1, 0)
    pl.semaphore_wait(barrier, met)

    gated = (pre_ref[...].astype(f32) * value_ref[...].astype(f32)).astype(bf16)
    tail[...] = gated[seq - 16 :]
    rim_copy = remote(tail, rim, rim_sem.at[0], rim_sem.at[1], at(sp + 1, tp))

    @pl.when(sp < sp_count - 1)
    def _():
        rim_copy.start()

    expert = lax.broadcasted_iota(jnp.int32, (sp_count, seq), 0)
    spread = jnp.zeros((sp_count, seq), f32)
    for k in range(ids_ref.shape[0]):
        spread = spread + jnp.where(expert == ids_ref[k : k + 1, :], weight_ref[k : k + 1, :], 0.0)
    scales[sp] = spread

    routes = (
        lambda group: (lax.div(group, 2) <= z) & (z < last),
        lambda group: (lax.div(group, 2) >= z) & (z > 0),
    )
    devices = (at(sp + 2, tp), at(sp - 2, tp), at(across, tp), at(sp, sibling), at(sp, opposite))

    def scale_copy(way, group):
        return remote(scales.at[group], scales.at[group], scale_send.at[way, group], scale_recv.at[group], devices[way])

    def send_scales(group):
        for way in range(2):

            @pl.when(routes[way](group))
            def _():
                scale_copy(way, group).start()

        scale_copy(2, group).start()

    send_scales(sp)
    padded[8:, :] = gated.astype(f32)

    @pl.when(sp == 0)
    def _():
        padded[:8, :] = jnp.zeros((8, padded.shape[1]), f32)

    @pl.when(sp > 0)
    def _():
        rim_copy.wait_recv()
        padded[:8, :] = rim[...].astype(f32)[8:]

    tap_count = taps_ref.shape[0]
    taps = taps_ref[...].astype(f32)
    convolved = jnp.zeros((seq, padded.shape[1]), f32)
    for k in range(tap_count):
        first = 8 - tap_count + 1 + k
        convolved = convolved + taps[k : k + 1, :] * padded[first : first + seq, :]
    mixed[...] = (post_ref[...].astype(f32) * convolved).astype(bf16)
    loads[0].wait()

    def rows_of(core):
        return jnp.concatenate(
            [mixed[pl.ds(pl.multiple_of(yy * half + core * rows, rows), rows), :] for yy in range(2)], 0
        )

    pair_send[...] = jnp.dot(rows_of(1 - c), out_w[...], preferred_element_type=f32).astype(bf16)
    pair_copy = remote(pair_send, pair_in, pair_sem.at[0], pair_sem.at[1], at(sp, sibling))
    pair_copy.start()
    own_sum[...] = jnp.dot(rows_of(c), out_w[...], preferred_element_type=f32)
    pair_copy.wait()
    far = pl.ds(pl.multiple_of((1 - y) * rows, rows), rows)
    near = pl.ds(pl.multiple_of(y * rows, rows), rows)
    y_send[...] = (own_sum[far, :] + pair_in[far, :].astype(f32)).astype(bf16)

    def y_copy(p):
        piece = pl.ds(p * step, step)
        return remote(y_send.at[piece, :], y_in.at[piece, :], y_sem.at[0], y_recv.at[p], at(sp, opposite))

    for p in range(PIECES):
        y_copy(p).start()
    own_sum[near, :] = own_sum[near, :] + pair_in[near, :].astype(f32)

    def height_of(relative):
        inner = jnp.where(relative == 0, 0, jnp.where(relative == 1, -1, relative - 1))
        return z + toward * jnp.where(at_end, relative, inner)

    def wait_scales(group):
        scale_copy(2, group).wait_recv()

    def take_scales(relative, carry):
        group = 2 * height_of(relative) + x
        wait_scales(group)
        send_scales(group)
        return carry

    lax.fori_loop(1, heights, take_scales, 0)

    def take_scales_across(height, carry):
        wait_scales(2 * height + 1 - x)
        return carry

    lax.fori_loop(0, heights, take_scales_across, 0)

    def piece_of(group, yy, p):
        return tokens.at[group, pl.ds(pl.multiple_of((2 * yy + c) * rows + p * step, step), step), :]

    def block_of(group, yy, core):
        return tokens.at[group, pl.ds(pl.multiple_of((2 * yy + core) * rows, rows), rows), :]

    def pass_on(way, group, yy, p):
        piece = piece_of(group, yy, p)
        receive = mate_recv.at[group, yy] if way == 3 else tok_recv.at[group, yy, p]
        return remote(piece, piece, tok_send.at[way, group, yy], receive, devices[way])

    def sent(way, group, yy):
        block = block_of(group, yy, c)
        return remote(block, block, tok_send.at[way, group, yy], mate_recv.at[group, yy], devices[way])

    def along_z(group, yy, p):
        for way in range(2):

            @pl.when(routes[way](group))
            def _():
                pass_on(way, group, yy, p).start()

    for p in range(PIECES):
        y_copy(p).wait_recv()
        piece = pl.ds(p * step, step)
        own = pl.ds(pl.multiple_of(y * rows + p * step, step), step)
        residual = (
            stream_ref[piece, :].astype(f32) + (own_sum[own, :] + y_in[piece, :].astype(f32))
        ).astype(bf16)
        resid[piece, :] = residual
        tokens[sp, pl.ds(pl.multiple_of(tp * rows + p * step, step), step), :] = scaled_norm(
            residual.astype(f32), gain_ref[...].reshape(1, width)
        ).astype(bf16)
        pass_on(4, sp, y, p).start()
        along_z(sp, y, p)
        pass_on(2, sp, y, p).start()
        pass_on(3, sp, y, p).start()

    for load in loads[1:]:
        load.wait()

    def wait_piece(group, yy, p):
        pass_on(2, group, yy, p).wait_recv()

    def wait_mate(group, yy):
        block = block_of(group, yy, 1 - c)
        remote(block, block, tok_send.at[3, group, yy], mate_recv.at[group, yy], at(sp, sibling)).wait_recv()

    def block_at(code):
        relative, second, p = lax.div(code, 2 * PIECES), lax.rem(lax.div(code, PIECES), 2), lax.rem(code, PIECES)
        return relative, height_of(relative), jnp.where(second == 0, y, 1 - y), p

    def take(code):
        relative, height, yy, p = block_at(code)
        group = 2 * height + x
        wait_piece(group, yy, p)

        @pl.when((relative > 0) | at_end)
        def _():
            along_z(group, yy, p)

        pass_on(3, group, yy, p).start()

        @pl.when(relative > 0)
        def _():
            pass_on(2, group, yy, p).start()

    def take_across(code):
        _, height, yy, p = block_at(code)
        group = 2 * height + 1 - x
        wait_piece(group, yy, p)
        pass_on(3, group, yy, p).start()

    def pass_held(code):
        p = lax.rem(code, PIECES)

        @pl.when(code < PIECES)
        def _():
            pass_on(2, sp, 1 - y, p).start()

        @pl.when(code >= PIECES)
        def _():
            along_z(sp, 1 - y, p)

    def tile_at(tile):
        height = height_of(lax.div(tile, 4))
        side = jnp.where(lax.rem(lax.div(tile, 2), 2) == 0, x, 1 - x)
        return height, 2 * height + side, jnp.where(lax.rem(tile, 2) == 0, y, 1 - y)

    def tile_rows(yy):
        return pl.ds(pl.multiple_of(yy * half, half), half)

    def share(way, group, yy):
        whose = tp if way < 2 else opposite
        block = hidden.at[group, whose, tile_rows(yy), :]
        return remote(
            block,
            block,
            hid_send.at[way, group, yy],
            hid_recv.at[group, whose, yy],
            at(sp, sibling if way else opposite),
        )

    def wait_shared(group, whose, yy):
        block = hidden.at[group, whose, tile_rows(yy), :]
        remote(block, block, hid_send.at[0, group, yy], hid_recv.at[group, whose, yy], at(sp, sibling)).wait_recv()

    def gated_units(tile):
        _, group, yy = tile_at(tile)
        wait_mate(group, yy)
        inputs = tokens[group, tile_rows(yy), :]
        span = min(256, units)
        for start in range(0, units, span):
            gate_pre = jnp.dot(inputs, gate_w[:, start : start + span], preferred_element_type=f32)
            up_pre = jnp.dot(inputs, up_w[:, start : start + span], preferred_element_type=f32)
            hidden[group, tp, tile_rows(yy), start : start + span] = clamped_units(gate_pre, up_pre).astype(bf16)
        share(0, group, yy).start()
        share(1, group, yy).start()

    def relay_units(tile):
        _, group, yy = tile_at(tile)
        wait_shared(group, opposite, yy)
        share(2, group, yy).start()

    def chain_copy(group, yy):
        rising = lax.div(group, 2) > z
        return remote(
            part.at[group, tile_rows(yy), :],
            chain_in.at[jnp.where(rising, 0, 1), group, tile_rows(yy), :],
            chain_send.at[group, yy],
            chain_recv.at[jnp.where(rising, 0, 1), group, yy],
            at(sp + jnp.where(rising, 2, -2), tp),
        )

    def wait_chain(side, group, yy):
        block = chain_in.at[side, group, tile_rows(yy), :]
        remote(
            block, block, chain_send.at[group, yy], chain_recv.at[side, group, yy], at(sp, sibling)
        ).wait_recv()

    diagonal = lax.broadcasted_iota(jnp.int32, (half, half), 0) == lax.broadcasted_iota(jnp.int32, (half, half), 1)

    def project_down(tile):
        height, group, yy = tile_at(tile)
        wait_shared(group, sibling, yy)
        wait_shared(group, 3 - tp, yy)
        own_rows = tile_rows(yy)
        out = jnp.dot(hidden[group, 0, own_rows, :], down_w[:units, :], preferred_element_type=f32)
        for k in range(1, 4):
            out = out + jnp.dot(
                hidden[group, k, own_rows, :], down_w[k * units : (k + 1) * units, :], preferred_element_type=f32
            )
        weight = scales[group, :, tile_rows(yy)]
        mine = lax.broadcasted_iota(jnp.int32, weight.shape, 0) == sp
        weight = jnp.sum(jnp.where(mine, weight, 0.0), axis=0, keepdims=True)
        weight = jnp.sum(jnp.where(diagonal, weight, 0.0), axis=1, keepdims=True)
        part[group, own_rows, :] = (out.astype(bf16).astype(f32) * weight).astype(bf16)

        @pl.when(((height > z) & (z == 0)) | ((height < z) & (z == last)))
        def _():
            chain_copy(group, yy).start()

    def x_copy(group, yy):
        return remote(
            part.at[group, tile_rows(yy), :], x_in.at[tile_rows(yy), :], x_send.at[yy], x_recv.at[yy], at(across, tp)
        )

    def hand_over(to):
        return remote(
            final.at[pl.ds(to * rows, rows), :], columns.at[tp], fin_send.at[to], fin_recv.at[tp], at(sp, to)
        )

    def toward_home(tile):
        height, group, yy = tile_at(tile)
        own_rows = tile_rows(yy)
        total[...] = part[group, own_rows, :].astype(f32)
        for side, comes in enumerate(((height >= z) & (z > 0), (height <= z) & (z < last))):

            @pl.when(comes)
            def _():
                wait_chain(side, group, yy)
                total[...] = total[...] + chain_in[side, group, own_rows, :].astype(f32)

        @pl.when(group != sp)
        def _():
            part[group, own_rows, :] = total[...].astype(bf16)

            @pl.when(height != z)
            def _():
                chain_copy(group, yy).start()

            @pl.when(height == z)
            def _():
                x_copy(group, yy).start()

        @pl.when(group == sp)
        def _():
            x_copy(group, yy).wait_recv()
            final[own_rows, :] = (total[...] + x_in[own_rows, :].astype(f32)).astype(bf16)
            for to in range(4):

                @pl.when((tp != to) & (yy == to // 2))
                def _():
                    hand_over(to).start()

    acts = (take, take_across, pass_held, gated_units, relay_units, project_down, toward_home)

    def four_events(position, carry):
        word = pick(at_end, plans, position)

        def event(i, carry):
            code = lax.shift_right_logical(word, 8 * i) & 255
            kind, rest = lax.div(code, 32), lax.rem(code, 32)
            for j, act in enumerate(acts):

                @pl.when(kind == j)
                def _():
                    act(rest)

            return carry

        return lax.fori_loop(0, 4, event, carry)

    plans = [words_of(plan) for plan in (end_plan, middle_plan)]
    lax.fori_loop(0, max(len(plan) for plan in plans), four_events, 0)

    columns[tp] = final[pl.ds(pl.multiple_of(tp * rows, rows), rows), :]
    for by in (1, 2, 3):
        whose = lax.rem(tp + by, 4)
        remote(
            final.at[pl.ds(0, rows), :], columns.at[whose], fin_send.at[0], fin_recv.at[whose], at(sp, sibling)
        ).wait_recv()
    combined = jnp.concatenate([columns[k] for k in range(4)], 1).astype(f32)
    result_ref[...] = (
        resid[...].astype(f32) + scaled_norm(combined, post_gain_ref[...].reshape(1, width))
    ).astype(bf16)

    @pl.when(sp < sp_count - 1)
    def _():
        rim_copy.wait_send()

    remote(y_send, y_in, y_sem.at[0], y_recv.at[0], at(sp, opposite)).wait_send()
    sent(4, sp, y).wait_send()
    for to in range(4):

        @pl.when(tp != to)
        def _():
            hand_over(to).wait_send()

    def drain(group, carry):
        height = lax.div(group, 2)

        @pl.when(lax.rem(group, 2) == x)
        def _():
            for way in range(2):

                @pl.when(routes[way](group))
                def _():
                    scale_copy(way, group).wait_send()
                    for yy in range(2):
                        sent(way, group, yy).wait_send()

            scale_copy(2, group).wait_send()
            for yy in range(2):
                sent(2, group, yy).wait_send()

        for yy in range(2):
            sent(3, group, yy).wait_send()
            for way in range(3):
                share(way, group, yy).wait_send()

            @pl.when(height != z)
            def _():
                chain_copy(group, yy).wait_send()

            @pl.when((height == z) & (group != sp))
            def _():
                x_copy(group, yy).wait_send()

        return carry

    lax.fori_loop(0, sp_count, drain, 0)


def dense_layer(
    stream_in,
    pre_gate,
    value_in,
    post_gate,
    conv_taps,
    out_weight,
    route_ids,
    route_weight,
    ffn_gain,
    post_gain,
    gate_proj,
    up_proj,
    down_proj,
):
    sp_count = lax.axis_size("sp")
    rows, width = stream_in.shape
    seq, channels = pre_gate.shape
    units = gate_proj.shape[2]
    cols = down_proj.shape[2]
    bf16, f32 = jnp.bfloat16, jnp.float32
    dma = pltpu.SemaphoreType.DMA
    scratch = [
        pltpu.VMEM(out_weight.shape, bf16),
        pltpu.VMEM(gate_proj.shape[1:], bf16),
        pltpu.VMEM(up_proj.shape[1:], bf16),
        pltpu.VMEM(down_proj.shape[1:], bf16),
        pltpu.VMEM((16, channels), bf16),
        pltpu.VMEM((16, channels), bf16),
        pltpu.VMEM((seq + 8, channels), f32),
        pltpu.VMEM((seq, channels), bf16),
        pltpu.VMEM((2 * rows, width), bf16),
        pltpu.VMEM((2 * rows, width), bf16),
        pltpu.VMEM((2 * rows, width), f32),
        pltpu.VMEM((rows, width), bf16),
        pltpu.VMEM((rows, width), bf16),
        pltpu.VMEM((rows, width), bf16),
        pltpu.VMEM((sp_count, sp_count, seq), f32),
        pltpu.VMEM((sp_count, seq, width), bf16),
        pltpu.VMEM((sp_count, 4, seq, units), bf16),
        pltpu.VMEM((sp_count, seq, cols), bf16),
        pltpu.VMEM((2, sp_count, seq, cols), bf16),
        pltpu.VMEM((seq, cols), bf16),
        pltpu.VMEM((2 * rows, cols), f32),
        pltpu.VMEM((seq, cols), bf16),
        pltpu.VMEM((4, rows, cols), bf16),
        dma((4,)),
        dma((2,)),
        dma((2,)),
        dma((1,)),
        dma((PIECES,)),
        dma((3, sp_count)),
        dma((sp_count,)),
        dma((5, sp_count, 2)),
        dma((sp_count, 2, PIECES)),
        dma((sp_count, 2)),
        dma((3, sp_count, 2)),
        dma((sp_count, 4, 2)),
        dma((sp_count, 2)),
        dma((2, sp_count, 2)),
        dma((2,)),
        dma((2,)),
        dma((4,)),
        dma((4,)),
    ]
    vmem = pl.BlockSpec(memory_space=pltpu.VMEM)
    anywhere = pl.BlockSpec(memory_space=pl.ANY)
    return pl.pallas_call(
        functools.partial(layer_kernel, sp_count),
        out_shape=jax.ShapeDtypeStruct((rows, width), bf16),
        in_specs=[vmem] * 9 + [anywhere] * 4,
        out_specs=vmem,
        scratch_shapes=scratch,
        compiler_params=pltpu.CompilerParams(
            collective_id=0, has_side_effects=True, vmem_limit_bytes=58 * 1024 * 1024
        ),
    )(
        stream_in,
        pre_gate,
        value_in,
        post_gate,
        conv_taps,
        route_ids.T,
        route_weight.T,
        ffn_gain,
        post_gain,
        out_weight,
        gate_proj,
        up_proj,
        down_proj,
    )


def local(
    stream_in,
    pre_gate,
    value_in,
    post_gate,
    conv_taps,
    out_weight,
    route_ids,
    route_weight,
    ffn_gain,
    post_gain,
    gate_proj,
    up_proj,
    down_proj,
):
    sp_count = lax.axis_size("sp")
    tp_count = lax.axis_size("tp")
    seq_rows = pre_gate.shape[0]
    own_rows = seq_rows // tp_count
    top_count = route_ids.shape[1]
    slots_each = 2 * own_rows * top_count // sp_count
    if tp_count == 4 and sp_count == PLANNED_GROUPS and slots_each >= own_rows:
        return dense_layer(
            stream_in, pre_gate, value_in, post_gate, conv_taps, out_weight, route_ids, route_weight,
            ffn_gain, post_gain, gate_proj, up_proj, down_proj,
        )
    tap_count = conv_taps.shape[0]
    gated_input = (pre_gate.astype(jnp.float32) * value_in.astype(jnp.float32)).astype(jnp.bfloat16)
    rim_rows = passed_along(gated_input[seq_rows - tap_count + 1 :], "sp", 1)
    padded = jnp.concatenate([rim_rows, gated_input], 0).astype(jnp.float32)
    convolved = jnp.zeros(gated_input.shape, jnp.float32)
    for tap_index in range(tap_count):
        convolved = (
            convolved
            + conv_taps[tap_index].astype(jnp.float32)[None, :]
            * padded[tap_index : tap_index + seq_rows]
        )
    mixer_out = (post_gate.astype(jnp.float32) * convolved).astype(jnp.bfloat16)
    weight_rows = mixer_out
    projected = lax.psum_scatter(
        jnp.dot(weight_rows, out_weight, preferred_element_type=jnp.float32),
        "tp",
        scatter_dimension=0,
        tiled=True,
    )
    residual = (stream_in.astype(jnp.float32) + projected).astype(jnp.bfloat16)
    normed = scaled_norm(residual.astype(jnp.float32), ffn_gain).astype(jnp.bfloat16)
    slot_rank = block_ranks(route_ids, sp_count, own_rows)
    block_of = (jnp.arange(seq_rows, dtype=jnp.int32) // own_rows)[:, None]
    tp_index = lax.axis_index("tp")
    own_ids = lax.dynamic_slice_in_dim(route_ids, tp_index * own_rows, own_rows, 0)
    own_rank = lax.dynamic_slice_in_dim(slot_rank, tp_index * own_rows, own_rows, 0)
    own_slot = own_ids * slots_each + own_rank
    picker = slot_picker(own_slot, sp_count * slots_each)
    outgoing = jnp.dot(picker, normed, preferred_element_type=jnp.float32).astype(jnp.bfloat16)
    arrived = lax.all_to_all(outgoing, "sp", split_axis=0, concat_axis=0, tiled=True)
    portion = lax.all_gather(arrived, "tp", axis=0, tiled=True)
    gate_pre = jnp.dot(portion, gate_proj[0], preferred_element_type=jnp.float32)
    up_pre = jnp.dot(portion, up_proj[0], preferred_element_type=jnp.float32)
    hidden = clamped_units(gate_pre, up_pre).astype(jnp.bfloat16)
    weight_rows = down_proj[0]
    column_out = jnp.dot(
        lax.all_gather(hidden, "tp", axis=1, tiled=True),
        weight_rows,
        preferred_element_type=jnp.float32,
    ).astype(jnp.bfloat16)
    column_width = column_out.shape[1]
    returned = lax.all_to_all(
        column_out.reshape(tp_count, sp_count, slots_each, column_width),
        "sp",
        split_axis=1,
        concat_axis=1,
        tiled=True,
    )
    home_index = (block_of * sp_count + route_ids) * slots_each + slot_rank
    gathered_out = jnp.take(returned.reshape(-1, column_width), home_index.reshape(-1), axis=0)
    gathered_out = gathered_out.astype(jnp.float32).reshape(seq_rows, top_count, column_width)
    combined_cols = jnp.sum(gathered_out * route_weight[:, :, None], axis=1).astype(jnp.bfloat16)
    combined = lax.all_to_all(combined_cols, "tp", split_axis=0, concat_axis=1, tiled=True)
    layer_out = residual.astype(jnp.float32) + scaled_norm(combined.astype(jnp.float32), post_gain)
    return layer_out.astype(jnp.bfloat16)


def solution(mesh):
    placed = (
        P(("sp", "tp"), None),
        P("sp", "tp"),
        P("sp", "tp"),
        P("sp", "tp"),
        P(None, "tp"),
        P("tp", None),
        P("sp", None),
        P("sp", None),
        P(),
        P(),
        P("sp", None, "tp"),
        P("sp", None, "tp"),
        P("sp", None, "tp"),
    )
    return jax.shard_map(
        local, mesh=mesh, in_specs=placed, out_specs=P(("sp", "tp"), None), check_vma=False
    )
```

```python
import functools

import jax
import jax.numpy as jnp
from jax import lax
from jax.experimental import pallas as pl
from jax.experimental.pallas import tpu as pltpu
from jax.sharding import PartitionSpec as P

clamp_limit = 7.0
sigmoid_scale = 1.702
epsilon = 1e-06


def passed_along(array, axis, by):
    count = lax.axis_size(axis)
    pairs = [(i, i + by) for i in range(count) if 0 <= i + by < count]
    return lax.ppermute(array, axis, pairs)


def clamped_units(gate_pre, up_pre):
    gate_cut = jnp.minimum(gate_pre, clamp_limit)
    up_cut = jnp.clip(up_pre, -clamp_limit, clamp_limit)
    return (up_cut + 1.0) * (gate_cut * jax.nn.sigmoid(sigmoid_scale * gate_cut))


def scaled_norm(values, gain):
    return (
        values
        * lax.rsqrt(jnp.mean(values * values, axis=-1, keepdims=True) + epsilon)
        * gain.astype(jnp.float32)
    )


def block_ranks(route_rows, experts, block_rows):
    flattened = route_rows.reshape(-1)
    entries = flattened.shape[0]
    span_width = block_rows * route_rows.shape[1]
    onehot = (flattened[:, None] == jnp.arange(experts, dtype=jnp.int32)[None, :]).astype(jnp.int32)
    blocked = onehot.reshape(entries // span_width, span_width, experts)
    before = jnp.cumsum(blocked, axis=1) - blocked
    return jnp.sum(before * blocked, axis=2).reshape(route_rows.shape)


def slot_picker(slot_index, table_size):
    matches = slot_index[None, :, :] == jnp.arange(table_size, dtype=jnp.int32)[:, None, None]
    return jnp.any(matches, axis=2).astype(jnp.bfloat16)


PIECES = 4
PLANNED_GROUPS = 8
end_plan = (
    32, 33, 4, 8, 10, 5, 96, 11, 35, 6, 16, 7, 34, 18, 98, 19, 43, 9, 17, 97,
    104, 26, 24, 48, 25, 27, 51, 49, 42, 41, 40, 50, 131, 108, 31, 28, 106, 30, 29, 66,
    58, 57, 64, 109, 56, 59, 137, 141, 110, 173, 60, 63, 62, 67, 61, 65, 140, 111, 172, 22,
    38, 23, 102, 143, 129, 39, 21, 20, 36, 15, 175, 142, 105, 55, 37, 174, 13, 12, 99, 53,
    54, 52, 139, 135, 14, 169, 107, 128, 136, 101, 171, 161, 130, 44, 168, 47, 45, 163, 46, 138,
    103, 170, 100, 160, 167, 162, 134, 132, 166, 194, 133, 164, 165, 195, 192, 193,
)
middle_plan = (
    9, 8, 16, 18, 96, 19, 10, 17, 4, 34, 104, 24, 11, 26, 5, 6, 7, 12, 14, 15,
    13, 25, 27, 100, 28, 108, 101, 31, 49, 51, 50, 48, 30, 29, 71, 109, 106, 68, 69, 97,
    33, 70, 58, 47, 46, 141, 140, 44, 45, 23, 32, 22, 20, 21, 103, 137, 133, 59, 56, 105,
    172, 57, 35, 165, 173, 60, 62, 63, 61, 40, 41, 111, 110, 136, 139, 42, 55, 43, 204, 129,
    205, 132, 52, 54, 169, 65, 66, 64, 67, 142, 53, 102, 168, 174, 128, 134, 107, 143, 206, 166,
    38, 197, 175, 135, 207, 171, 98, 167, 198, 37, 39, 36, 160, 138, 203, 161, 99, 199, 164, 170,
    196, 202, 131, 163, 195, 130, 201, 162, 200, 194, 192, 193,
)

def words_of(plan):
    codes = list(plan)
    codes += [255] * (-len(codes) % 4)
    words = [sum(code << (8 * i) for i, code in enumerate(codes[at : at + 4])) for at in range(0, len(codes), 4)]
    return [word - (1 << 32) if word >> 31 else word for word in words]


def pick(at_end, tables, position):
    value = jnp.int32(-1)
    for i, table in enumerate(tables):
        chosen = jnp.int32(-1)
        for j, word in enumerate(table):
            chosen = jnp.where(position == j, word, chosen)
        value = jnp.where(at_end == (i == 0), chosen, value)
    return value


def layer_kernel(
    sp_count,
    stream_ref,
    pre_ref,
    value_ref,
    post_ref,
    taps_ref,
    ids_ref,
    weight_ref,
    gain_ref,
    post_gain_ref,
    out_hbm,
    gate_hbm,
    up_hbm,
    down_hbm,
    result_ref,
    out_w,
    gate_w,
    up_w,
    down_w,
    tail,
    rim,
    padded,
    mixed,
    pair_send,
    pair_in,
    own_sum,
    y_send,
    y_in,
    resid,
    scales,
    tokens,
    hidden,
    part,
    chain_in,
    x_in,
    total,
    final,
    columns,
    load_sem,
    rim_sem,
    pair_sem,
    y_sem,
    y_recv,
    scale_send,
    scale_recv,
    tok_send,
    tok_recv,
    mate_recv,
    hid_send,
    hid_recv,
    mate_hid_recv,
    chain_send,
    chain_recv,
    x_send,
    x_recv,
    fin_send,
    fin_recv,
):
    f32, bf16 = jnp.float32, jnp.bfloat16
    heights = sp_count // 2
    last = heights - 1
    sp = lax.axis_index("sp")
    tp = lax.axis_index("tp")
    z, x = lax.div(sp, 2), lax.rem(sp, 2)
    y, c = lax.div(tp, 2), lax.rem(tp, 2)
    across, sibling = sp + 1 - 2 * x, tp + 1 - 2 * c
    opposite = lax.rem(tp + 2, 4)
    rows, width = stream_ref.shape
    seq = 4 * rows
    half = 2 * rows
    step = rows // PIECES
    units = gate_w.shape[1]
    at_end = (z == 0) | (z == last)
    toward = jnp.where(2 * z < heights, 1, -1)

    def at(sp_to, tp_to):
        return {"sp": sp_to, "tp": tp_to}

    def remote(source, target, send, receive, device):
        return pltpu.make_async_remote_copy(
            src_ref=source,
            dst_ref=target,
            send_sem=send,
            recv_sem=receive,
            device_id=device,
            device_id_type=pl.DeviceIdType.MESH,
        )

    loads = [
        pltpu.make_async_copy(source, target, load_sem.at[i])
        for i, (source, target) in enumerate(
            ((out_hbm, out_w), (gate_hbm.at[0], gate_w), (up_hbm.at[0], up_w), (down_hbm.at[0], down_w))
        )
    ]
    for load in loads:
        load.start()

    barrier = pltpu.get_barrier_semaphore()

    def greet(partner):
        pl.semaphore_signal(barrier, inc=1, device_id=partner, device_id_type=pl.DeviceIdType.MESH)

    for partner in (at(across, tp), at(sp, sibling), at(sp, opposite), at(sp, 3 - tp)):
        greet(partner)
    met = jnp.int32(4)
    for there, by in ((sp < sp_count - 1, 1), (sp > 0, -1), (z < last, 2), (z > 0, -2)):

        @pl.when(there)
        def _():
            greet(at(sp + by, tp))

        met = met + jnp.where(there, 1, 0)
    pl.semaphore_wait(barrier, met)

    gated = (pre_ref[...].astype(f32) * value_ref[...].astype(f32)).astype(bf16)
    tail[...] = gated[seq - 16 :]
    rim_copy = remote(tail, rim, rim_sem.at[0], rim_sem.at[1], at(sp + 1, tp))

    @pl.when(sp < sp_count - 1)
    def _():
        rim_copy.start()

    expert = lax.broadcasted_iota(jnp.int32, (sp_count, seq), 0)
    spread = jnp.zeros((sp_count, seq), f32)
    for k in range(ids_ref.shape[0]):
        spread = spread + jnp.where(expert == ids_ref[k : k + 1, :], weight_ref[k : k + 1, :], 0.0)
    scales[sp] = spread

    routes = (
        lambda group: (lax.div(group, 2) <= z) & (z < last),
        lambda group: (lax.div(group, 2) >= z) & (z > 0),
    )
    devices = (at(sp + 2, tp), at(sp - 2, tp), at(across, tp), at(sp, sibling), at(sp, opposite))

    def scale_copy(way, group):
        return remote(scales.at[group], scales.at[group], scale_send.at[way], scale_recv.at[group], devices[way])

    def send_scales(group):
        for way in range(2):

            @pl.when(routes[way](group))
            def _():
                scale_copy(way, group).start()

        scale_copy(2, group).start()

    send_scales(sp)
    padded[8:, :] = gated.astype(f32)

    @pl.when(sp == 0)
    def _():
        padded[:8, :] = jnp.zeros((8, padded.shape[1]), f32)

    @pl.when(sp > 0)
    def _():
        rim_copy.wait_recv()
        padded[:8, :] = rim[...].astype(f32)[8:]

    tap_count = taps_ref.shape[0]
    taps = taps_ref[...].astype(f32)
    convolved = jnp.zeros((seq, padded.shape[1]), f32)
    for k in range(tap_count):
        first = 8 - tap_count + 1 + k
        convolved = convolved + taps[k : k + 1, :] * padded[first : first + seq, :]
    mixed[...] = (post_ref[...].astype(f32) * convolved).astype(bf16)
    loads[0].wait()

    def rows_of(core):
        return jnp.concatenate(
            [mixed[pl.ds(pl.multiple_of(yy * half + core * rows, rows), rows), :] for yy in range(2)], 0
        )

    pair_send[...] = jnp.dot(rows_of(1 - c), out_w[...], preferred_element_type=f32).astype(bf16)
    pair_copy = remote(pair_send, pair_in, pair_sem.at[0], pair_sem.at[1], at(sp, sibling))
    pair_copy.start()
    own_sum[...] = jnp.dot(rows_of(c), out_w[...], preferred_element_type=f32)
    pair_copy.wait()
    far = pl.ds(pl.multiple_of((1 - y) * rows, rows), rows)
    near = pl.ds(pl.multiple_of(y * rows, rows), rows)
    y_send[...] = (own_sum[far, :] + pair_in[far, :].astype(f32)).astype(bf16)

    def y_copy(p):
        piece = pl.ds(p * step, step)
        return remote(y_send.at[piece, :], y_in.at[piece, :], y_sem.at[0], y_recv.at[p], at(sp, opposite))

    for p in range(PIECES):
        y_copy(p).start()
    own_sum[near, :] = own_sum[near, :] + pair_in[near, :].astype(f32)

    def height_of(relative):
        inner = jnp.where(relative == 0, 0, jnp.where(relative == 1, -1, relative - 1))
        return z + toward * jnp.where(at_end, relative, inner)

    def wait_scales(group):
        scale_copy(2, group).wait_recv()

    def piece_of(group, yy, p):
        return tokens.at[group, pl.ds(pl.multiple_of((2 * yy + c) * rows + p * step, step), step), :]

    def block_of(group, yy, core):
        return tokens.at[group, pl.ds(pl.multiple_of((2 * yy + core) * rows, rows), rows), :]

    def pass_on(way, group, yy, p):
        piece = piece_of(group, yy, p)
        receive = mate_recv.at[group, yy] if way == 3 else tok_recv.at[group, yy, p]
        return remote(piece, piece, tok_send.at[way], receive, devices[way])

    def sent(way, group_count, row_count):
        rows_sent = tokens.at[pl.ds(0, group_count), pl.ds(0, row_count), :]
        return remote(rows_sent, rows_sent, tok_send.at[way], mate_recv.at[0, 0], devices[way])

    def along_z(group, yy, p):
        for way in range(2):

            @pl.when(routes[way](group))
            def _():
                pass_on(way, group, yy, p).start()

    for p in range(PIECES):
        y_copy(p).wait_recv()
        piece = pl.ds(p * step, step)
        own = pl.ds(pl.multiple_of(y * rows + p * step, step), step)
        residual = (
            stream_ref[piece, :].astype(f32) + (own_sum[own, :] + y_in[piece, :].astype(f32))
        ).astype(bf16)
        resid[piece, :] = residual
        tokens[sp, pl.ds(pl.multiple_of(tp * rows + p * step, step), step), :] = scaled_norm(
            residual.astype(f32), gain_ref[...].reshape(1, width)
        ).astype(bf16)
        pass_on(4, sp, y, p).start()
        along_z(sp, y, p)
        pass_on(2, sp, y, p).start()
        pass_on(3, sp, y, p).start()

    for load in loads[1:]:
        load.wait()

    def wait_piece(group, yy, p):
        pass_on(2, group, yy, p).wait_recv()

    def wait_mate(group, yy):
        block = block_of(group, yy, 1 - c)
        remote(block, block, tok_send.at[3], mate_recv.at[group, yy], at(sp, sibling)).wait_recv()

    def block_at(code):
        relative, second, p = lax.div(code, 2 * PIECES), lax.rem(lax.div(code, PIECES), 2), lax.rem(code, PIECES)
        return relative, height_of(relative), jnp.where(second == 0, y, 1 - y), p

    def take(code):
        relative, height, yy, p = block_at(code)
        group = 2 * height + x

        @pl.when((relative > 0) & (lax.rem(code, 2 * PIECES) == 0))
        def _():
            wait_scales(group)
            send_scales(group)

        wait_piece(group, yy, p)

        @pl.when((relative > 0) | at_end)
        def _():
            along_z(group, yy, p)

        pass_on(3, group, yy, p).start()

        @pl.when(relative > 0)
        def _():
            pass_on(2, group, yy, p).start()

    def take_across(code):
        _, height, yy, p = block_at(code)
        group = 2 * height + 1 - x

        @pl.when(lax.rem(code, 2 * PIECES) == 0)
        def _():
            wait_scales(group)

        wait_piece(group, yy, p)
        pass_on(3, group, yy, p).start()

    def pass_held(code):
        p = lax.rem(code, PIECES)

        @pl.when(code < PIECES)
        def _():
            pass_on(2, sp, 1 - y, p).start()

        @pl.when(code >= PIECES)
        def _():
            along_z(sp, 1 - y, p)

    def tile_at(tile):
        height = height_of(lax.div(tile, 4))
        side = jnp.where(lax.rem(lax.div(tile, 2), 2) == 0, x, 1 - x)
        return height, 2 * height + side, jnp.where(lax.rem(tile, 2) == 0, y, 1 - y)

    def tile_rows(yy):
        return pl.ds(pl.multiple_of(yy * half, half), half)

    def share(way, group, yy):
        whose = tp if way < 2 else opposite
        block = hidden.at[group, whose, tile_rows(yy), :]
        receive = mate_hid_recv.at[group, yy] if way else hid_recv.at[group, yy]
        return remote(block, block, hid_send.at[way], receive, at(sp, sibling if way else opposite))

    def gated_units(tile):
        _, group, yy = tile_at(tile)
        wait_mate(group, yy)
        inputs = tokens[group, tile_rows(yy), :]
        span = min(256, units)
        for start in range(0, units, span):
            gate_pre = jnp.dot(inputs, gate_w[:, start : start + span], preferred_element_type=f32)
            up_pre = jnp.dot(inputs, up_w[:, start : start + span], preferred_element_type=f32)
            hidden[group, tp, tile_rows(yy), start : start + span] = clamped_units(gate_pre, up_pre).astype(bf16)
        share(0, group, yy).start()
        share(1, group, yy).start()

    def relay_units(tile):
        _, group, yy = tile_at(tile)
        share(0, group, yy).wait_recv()
        share(2, group, yy).start()

    def chain_copy(group, yy):
        rising = lax.div(group, 2) > z
        return remote(
            part.at[group, tile_rows(yy), :],
            chain_in.at[jnp.where(rising, 0, 1), group, tile_rows(yy), :],
            chain_send.at[0],
            chain_recv.at[group, yy],
            at(sp + jnp.where(rising, 2, -2), tp),
        )

    def wait_chain(sides, group, yy):
        tiles = chain_in.at[pl.ds(0, sides), group, tile_rows(yy), :]
        remote(tiles, tiles, chain_send.at[0], chain_recv.at[group, yy], at(sp, sibling)).wait_recv()

    diagonal = lax.broadcasted_iota(jnp.int32, (half, half), 0) == lax.broadcasted_iota(jnp.int32, (half, half), 1)

    def project_down(tile):
        height, group, yy = tile_at(tile)
        both = hidden.at[group, pl.ds(0, 2), tile_rows(yy), :]
        remote(both, both, hid_send.at[1], mate_hid_recv.at[group, yy], at(sp, sibling)).wait_recv()
        own_rows = tile_rows(yy)
        out = jnp.dot(hidden[group, 0, own_rows, :], down_w[:units, :], preferred_element_type=f32)
        for k in range(1, 4):
            out = out + jnp.dot(
                hidden[group, k, own_rows, :], down_w[k * units : (k + 1) * units, :], preferred_element_type=f32
            )
        weight = scales[group, :, tile_rows(yy)]
        mine = lax.broadcasted_iota(jnp.int32, weight.shape, 0) == sp
        weight = jnp.sum(jnp.where(mine, weight, 0.0), axis=0, keepdims=True)
        weight = jnp.sum(jnp.where(diagonal, weight, 0.0), axis=1, keepdims=True)
        part[group, own_rows, :] = (out.astype(bf16).astype(f32) * weight).astype(bf16)

        @pl.when(((height > z) & (z == 0)) | ((height < z) & (z == last)))
        def _():
            chain_copy(group, yy).start()

    def x_copy(group, yy):
        return remote(
            part.at[group, tile_rows(yy), :], x_in.at[tile_rows(yy), :], x_send.at[0], x_recv.at[yy], at(across, tp)
        )

    def hand_over(to):
        return remote(
            final.at[pl.ds(to * rows, rows), :], columns.at[tp], fin_send.at[0], fin_recv.at[tp], at(sp, to)
        )

    def toward_home(tile):
        height, group, yy = tile_at(tile)
        own_rows = tile_rows(yy)
        total[...] = part[group, own_rows, :].astype(f32)
        both_sides = (height == z) & jnp.logical_not(at_end)

        @pl.when(both_sides)
        def _():
            wait_chain(2, group, yy)

        @pl.when(jnp.logical_not(both_sides))
        def _():
            wait_chain(1, group, yy)

        for side, comes in enumerate(((height >= z) & (z > 0), (height <= z) & (z < last))):

            @pl.when(comes)
            def _():
                total[...] = total[...] + chain_in[side, group, own_rows, :].astype(f32)

        @pl.when(group != sp)
        def _():
            part[group, own_rows, :] = total[...].astype(bf16)

            @pl.when(height != z)
            def _():
                chain_copy(group, yy).start()

            @pl.when(height == z)
            def _():
                x_copy(group, yy).start()

        @pl.when(group == sp)
        def _():
            x_copy(group, yy).wait_recv()
            final[own_rows, :] = (total[...] + x_in[own_rows, :].astype(f32)).astype(bf16)
            for to in range(4):

                @pl.when((tp != to) & (yy == to // 2))
                def _():
                    hand_over(to).start()

    acts = (take, take_across, pass_held, gated_units, relay_units, project_down, toward_home)

    def four_events(position, carry):
        word = pick(at_end, plans, position)

        def event(i, carry):
            code = lax.shift_right_logical(word, 8 * i) & 255
            kind, rest = lax.div(code, 32), lax.rem(code, 32)
            for j, act in enumerate(acts):

                @pl.when(kind == j)
                def _():
                    act(rest)

            return carry

        return lax.fori_loop(0, 4, event, carry)

    plans = [words_of(plan) for plan in (end_plan, middle_plan)]
    lax.fori_loop(0, max(len(plan) for plan in plans), four_events, 0)

    columns[tp] = final[pl.ds(pl.multiple_of(tp * rows, rows), rows), :]
    for by in (1, 2, 3):
        whose = lax.rem(tp + by, 4)
        remote(
            final.at[pl.ds(0, rows), :], columns.at[whose], fin_send.at[0], fin_recv.at[whose], at(sp, sibling)
        ).wait_recv()
    combined = jnp.concatenate([columns[k] for k in range(4)], 1).astype(f32)
    result_ref[...] = (
        resid[...].astype(f32) + scaled_norm(combined, post_gain_ref[...].reshape(1, width))
    ).astype(bf16)

    @pl.when(sp < sp_count - 1)
    def _():
        rim_copy.wait_send()

    remote(y_send, y_in, y_sem.at[0], y_recv.at[0], at(sp, opposite)).wait_send()
    sent(4, 1, rows).wait_send()
    sent(3, heights, seq).wait_send()
    sent(2, heights, half).wait_send()

    def scales_sent(way, group_count):
        blocks = scales.at[pl.ds(0, group_count)]
        remote(blocks, blocks, scale_send.at[way], scale_recv.at[0], devices[way]).wait_send()

    scales_sent(2, heights)
    for count in range(1, heights):
        for way, its in enumerate((z == count - 1, z == heights - count)):

            @pl.when(its)
            def _():
                sent(way, count, half).wait_send()
                scales_sent(way, count)

    for way in range(3):
        tiles = hidden.at[:, 0]
        receive = mate_hid_recv.at[0, 0] if way else hid_recv.at[0, 0]
        remote(tiles, tiles, hid_send.at[way], receive, at(sp, sibling)).wait_send()
    chained = part.at[pl.ds(0, sp_count - 2)]
    remote(chained, chained, chain_send.at[0], chain_recv.at[0, 0], at(sp, sibling)).wait_send()
    remote(part.at[0], x_in, x_send.at[0], x_recv.at[0], at(across, tp)).wait_send()
    handed = final.at[pl.ds(0, 3 * rows), :]
    remote(handed, handed, fin_send.at[0], fin_recv.at[0], at(sp, sibling)).wait_send()


def dense_layer(
    stream_in,
    pre_gate,
    value_in,
    post_gate,
    conv_taps,
    out_weight,
    route_ids,
    route_weight,
    ffn_gain,
    post_gain,
    gate_proj,
    up_proj,
    down_proj,
):
    sp_count = lax.axis_size("sp")
    rows, width = stream_in.shape
    seq, channels = pre_gate.shape
    units = gate_proj.shape[2]
    cols = down_proj.shape[2]
    bf16, f32 = jnp.bfloat16, jnp.float32
    dma = pltpu.SemaphoreType.DMA
    scratch = [
        pltpu.VMEM(out_weight.shape, bf16),
        pltpu.VMEM(gate_proj.shape[1:], bf16),
        pltpu.VMEM(up_proj.shape[1:], bf16),
        pltpu.VMEM(down_proj.shape[1:], bf16),
        pltpu.VMEM((16, channels), bf16),
        pltpu.VMEM((16, channels), bf16),
        pltpu.VMEM((seq + 8, channels), f32),
        pltpu.VMEM((seq, channels), bf16),
        pltpu.VMEM((2 * rows, width), bf16),
        pltpu.VMEM((2 * rows, width), bf16),
        pltpu.VMEM((2 * rows, width), f32),
        pltpu.VMEM((rows, width), bf16),
        pltpu.VMEM((rows, width), bf16),
        pltpu.VMEM((rows, width), bf16),
        pltpu.VMEM((sp_count, sp_count, seq), f32),
        pltpu.VMEM((sp_count, seq, width), bf16),
        pltpu.VMEM((sp_count, 4, seq, units), bf16),
        pltpu.VMEM((sp_count, seq, cols), bf16),
        pltpu.VMEM((2, sp_count, seq, cols), bf16),
        pltpu.VMEM((seq, cols), bf16),
        pltpu.VMEM((2 * rows, cols), f32),
        pltpu.VMEM((seq, cols), bf16),
        pltpu.VMEM((4, rows, cols), bf16),
        dma((4,)),
        dma((2,)),
        dma((2,)),
        dma((1,)),
        dma((PIECES,)),
        dma((3,)),
        dma((sp_count,)),
        dma((5,)),
        dma((sp_count, 2, PIECES)),
        dma((sp_count, 2)),
        dma((3,)),
        dma((sp_count, 2)),
        dma((sp_count, 2)),
        dma((1,)),
        dma((sp_count, 2)),
        dma((1,)),
        dma((2,)),
        dma((1,)),
        dma((4,)),
    ]
    vmem = pl.BlockSpec(memory_space=pltpu.VMEM)
    anywhere = pl.BlockSpec(memory_space=pl.ANY)
    return pl.pallas_call(
        functools.partial(layer_kernel, sp_count),
        out_shape=jax.ShapeDtypeStruct((rows, width), bf16),
        in_specs=[vmem] * 9 + [anywhere] * 4,
        out_specs=vmem,
        scratch_shapes=scratch,
        compiler_params=pltpu.CompilerParams(
            collective_id=0, has_side_effects=True, vmem_limit_bytes=58 * 1024 * 1024
        ),
    )(
        stream_in,
        pre_gate,
        value_in,
        post_gate,
        conv_taps,
        route_ids.T,
        route_weight.T,
        ffn_gain,
        post_gain,
        out_weight,
        gate_proj,
        up_proj,
        down_proj,
    )


def local(
    stream_in,
    pre_gate,
    value_in,
    post_gate,
    conv_taps,
    out_weight,
    route_ids,
    route_weight,
    ffn_gain,
    post_gain,
    gate_proj,
    up_proj,
    down_proj,
):
    sp_count = lax.axis_size("sp")
    tp_count = lax.axis_size("tp")
    seq_rows = pre_gate.shape[0]
    own_rows = seq_rows // tp_count
    top_count = route_ids.shape[1]
    slots_each = 2 * own_rows * top_count // sp_count
    if tp_count == 4 and sp_count == PLANNED_GROUPS and slots_each >= own_rows:
        return dense_layer(
            stream_in, pre_gate, value_in, post_gate, conv_taps, out_weight, route_ids, route_weight,
            ffn_gain, post_gain, gate_proj, up_proj, down_proj,
        )
    tap_count = conv_taps.shape[0]
    gated_input = (pre_gate.astype(jnp.float32) * value_in.astype(jnp.float32)).astype(jnp.bfloat16)
    rim_rows = passed_along(gated_input[seq_rows - tap_count + 1 :], "sp", 1)
    padded = jnp.concatenate([rim_rows, gated_input], 0).astype(jnp.float32)
    convolved = jnp.zeros(gated_input.shape, jnp.float32)
    for tap_index in range(tap_count):
        convolved = (
            convolved
            + conv_taps[tap_index].astype(jnp.float32)[None, :]
            * padded[tap_index : tap_index + seq_rows]
        )
    mixer_out = (post_gate.astype(jnp.float32) * convolved).astype(jnp.bfloat16)
    weight_rows = mixer_out
    projected = lax.psum_scatter(
        jnp.dot(weight_rows, out_weight, preferred_element_type=jnp.float32),
        "tp",
        scatter_dimension=0,
        tiled=True,
    )
    residual = (stream_in.astype(jnp.float32) + projected).astype(jnp.bfloat16)
    normed = scaled_norm(residual.astype(jnp.float32), ffn_gain).astype(jnp.bfloat16)
    slot_rank = block_ranks(route_ids, sp_count, own_rows)
    block_of = (jnp.arange(seq_rows, dtype=jnp.int32) // own_rows)[:, None]
    tp_index = lax.axis_index("tp")
    own_ids = lax.dynamic_slice_in_dim(route_ids, tp_index * own_rows, own_rows, 0)
    own_rank = lax.dynamic_slice_in_dim(slot_rank, tp_index * own_rows, own_rows, 0)
    own_slot = own_ids * slots_each + own_rank
    picker = slot_picker(own_slot, sp_count * slots_each)
    outgoing = jnp.dot(picker, normed, preferred_element_type=jnp.float32).astype(jnp.bfloat16)
    arrived = lax.all_to_all(outgoing, "sp", split_axis=0, concat_axis=0, tiled=True)
    portion = lax.all_gather(arrived, "tp", axis=0, tiled=True)
    gate_pre = jnp.dot(portion, gate_proj[0], preferred_element_type=jnp.float32)
    up_pre = jnp.dot(portion, up_proj[0], preferred_element_type=jnp.float32)
    hidden = clamped_units(gate_pre, up_pre).astype(jnp.bfloat16)
    weight_rows = down_proj[0]
    column_out = jnp.dot(
        lax.all_gather(hidden, "tp", axis=1, tiled=True),
        weight_rows,
        preferred_element_type=jnp.float32,
    ).astype(jnp.bfloat16)
    column_width = column_out.shape[1]
    returned = lax.all_to_all(
        column_out.reshape(tp_count, sp_count, slots_each, column_width),
        "sp",
        split_axis=1,
        concat_axis=1,
        tiled=True,
    )
    home_index = (block_of * sp_count + route_ids) * slots_each + slot_rank
    gathered_out = jnp.take(returned.reshape(-1, column_width), home_index.reshape(-1), axis=0)
    gathered_out = gathered_out.astype(jnp.float32).reshape(seq_rows, top_count, column_width)
    combined_cols = jnp.sum(gathered_out * route_weight[:, :, None], axis=1).astype(jnp.bfloat16)
    combined = lax.all_to_all(combined_cols, "tp", split_axis=0, concat_axis=1, tiled=True)
    layer_out = residual.astype(jnp.float32) + scaled_norm(combined.astype(jnp.float32), post_gain)
    return layer_out.astype(jnp.bfloat16)


def solution(mesh):
    placed = (
        P(("sp", "tp"), None),
        P("sp", "tp"),
        P("sp", "tp"),
        P("sp", "tp"),
        P(None, "tp"),
        P("tp", None),
        P("sp", None),
        P("sp", None),
        P(),
        P(),
        P("sp", None, "tp"),
        P("sp", None, "tp"),
        P("sp", None, "tp"),
    )
    return jax.shard_map(
        local, mesh=mesh, in_specs=placed, out_specs=P(("sp", "tp"), None), check_vma=False
    )
```

```python
import functools

import jax
import jax.numpy as jnp
from jax import lax
from jax.experimental import pallas as pl
from jax.experimental.pallas import tpu as pltpu
from jax.sharding import PartitionSpec as P

clamp_limit = 7.0
sigmoid_scale = 1.702
epsilon = 1e-06


def passed_along(array, axis, by):
    count = lax.axis_size(axis)
    pairs = [(i, i + by) for i in range(count) if 0 <= i + by < count]
    return lax.ppermute(array, axis, pairs)


def clamped_units(gate_pre, up_pre):
    gate_cut = jnp.minimum(gate_pre, clamp_limit)
    up_cut = jnp.clip(up_pre, -clamp_limit, clamp_limit)
    return (up_cut + 1.0) * (gate_cut * jax.nn.sigmoid(sigmoid_scale * gate_cut))


def scaled_norm(values, gain):
    return (
        values
        * lax.rsqrt(jnp.mean(values * values, axis=-1, keepdims=True) + epsilon)
        * gain.astype(jnp.float32)
    )


def block_ranks(route_rows, experts, block_rows):
    flattened = route_rows.reshape(-1)
    entries = flattened.shape[0]
    span_width = block_rows * route_rows.shape[1]
    onehot = (flattened[:, None] == jnp.arange(experts, dtype=jnp.int32)[None, :]).astype(jnp.int32)
    blocked = onehot.reshape(entries // span_width, span_width, experts)
    before = jnp.cumsum(blocked, axis=1) - blocked
    return jnp.sum(before * blocked, axis=2).reshape(route_rows.shape)


def slot_picker(slot_index, table_size):
    matches = slot_index[None, :, :] == jnp.arange(table_size, dtype=jnp.int32)[:, None, None]
    return jnp.any(matches, axis=2).astype(jnp.bfloat16)


PIECES = 4
PLANNED_GROUPS = 8
end_plan = (
    8, 9, 11, 10, 34, 5, 6, 40, 96, 16, 4, 7, 43, 18, 97, 32, 33, 35, 19, 42,
    41, 98, 17, 26, 104, 27, 102, 25, 58, 24, 29, 59, 31, 129, 128, 30, 108, 28, 65, 64,
    66, 56, 67, 137, 48, 51, 50, 61, 57, 49, 109, 110, 106, 62, 141, 63, 173, 22, 140, 161,
    60, 172, 21, 111, 23, 143, 20, 175, 105, 13, 14, 131, 15, 54, 169, 39, 37, 53, 139, 142,
    12, 36, 38, 135, 55, 52, 174, 107, 99, 45, 136, 171, 47, 168, 46, 44, 163, 138, 103, 170,
    100, 160, 130, 101, 195, 162, 167, 134, 166, 133, 194, 165, 193, 132, 164, 192,
)
middle_plan = (
    16, 8, 17, 10, 96, 18, 19, 11, 9, 104, 26, 33, 24, 27, 100, 25, 5, 13, 42, 6,
    14, 15, 12, 4, 7, 108, 29, 30, 97, 31, 101, 28, 35, 32, 34, 70, 109, 59, 129, 56,
    58, 69, 57, 41, 71, 141, 133, 43, 110, 68, 22, 21, 50, 51, 23, 48, 49, 132, 140, 20,
    40, 102, 106, 44, 45, 60, 63, 61, 62, 46, 47, 173, 65, 66, 67, 143, 111, 172, 103, 55,
    54, 139, 175, 207, 52, 205, 53, 64, 164, 135, 165, 107, 142, 128, 167, 105, 171, 137, 38, 199,
    174, 206, 204, 36, 134, 37, 39, 138, 197, 98, 203, 99, 166, 198, 136, 170, 161, 202, 196, 131,
    169, 168, 160, 201, 130, 163, 195, 162, 194, 200, 193, 192,
)

def words_of(plan):
    codes = list(plan)
    codes += [255] * (-len(codes) % 4)
    words = [sum(code << (8 * i) for i, code in enumerate(codes[at : at + 4])) for at in range(0, len(codes), 4)]
    return [word - (1 << 32) if word >> 31 else word for word in words]


def pick(at_end, tables, position):
    value = jnp.int32(-1)
    for i, table in enumerate(tables):
        chosen = jnp.int32(-1)
        for j, word in enumerate(table):
            chosen = jnp.where(position == j, word, chosen)
        value = jnp.where(at_end == (i == 0), chosen, value)
    return value


def layer_kernel(
    sp_count,
    stream_ref,
    pre_ref,
    value_ref,
    post_ref,
    taps_ref,
    ids_ref,
    weight_ref,
    gain_ref,
    post_gain_ref,
    out_hbm,
    gate_hbm,
    up_hbm,
    down_hbm,
    result_ref,
    out_w,
    gate_w,
    up_w,
    down_w,
    tail,
    rim,
    padded,
    mixed,
    pair_send,
    pair_in,
    own_sum,
    y_send,
    y_in,
    resid,
    scales,
    tokens,
    hidden,
    part,
    chain_in,
    x_in,
    total,
    final,
    columns,
    load_sem,
    rim_sem,
    pair_sem,
    pair_recv,
    y_sem,
    y_recv,
    scale_send,
    scale_recv,
    tok_send,
    tok_recv,
    mate_recv,
    hid_send,
    hid_recv,
    mate_hid_recv,
    chain_send,
    chain_recv,
    x_send,
    x_recv,
    fin_send,
    fin_recv,
):
    f32, bf16 = jnp.float32, jnp.bfloat16
    heights = sp_count // 2
    last = heights - 1
    sp = lax.axis_index("sp")
    tp = lax.axis_index("tp")
    z, x = lax.div(sp, 2), lax.rem(sp, 2)
    y, c = lax.div(tp, 2), lax.rem(tp, 2)
    across, sibling = sp + 1 - 2 * x, tp + 1 - 2 * c
    opposite = lax.rem(tp + 2, 4)
    rows, width = stream_ref.shape
    seq = 4 * rows
    half = 2 * rows
    step = rows // PIECES
    units = gate_w.shape[1]
    at_end = (z == 0) | (z == last)
    toward = jnp.where(2 * z < heights, 1, -1)

    def at(sp_to, tp_to):
        return {"sp": sp_to, "tp": tp_to}

    def remote(source, target, send, receive, device):
        return pltpu.make_async_remote_copy(
            src_ref=source,
            dst_ref=target,
            send_sem=send,
            recv_sem=receive,
            device_id=device,
            device_id_type=pl.DeviceIdType.MESH,
        )

    loads = [
        pltpu.make_async_copy(source, target, load_sem.at[i])
        for i, (source, target) in enumerate(
            ((out_hbm, out_w), (gate_hbm.at[0], gate_w), (up_hbm.at[0], up_w), (down_hbm.at[0], down_w))
        )
    ]
    for load in loads:
        load.start()

    barrier = pltpu.get_barrier_semaphore()

    def greet(partner):
        pl.semaphore_signal(barrier, inc=1, device_id=partner, device_id_type=pl.DeviceIdType.MESH)

    for partner in (at(across, tp), at(sp, sibling), at(sp, opposite), at(sp, 3 - tp)):
        greet(partner)
    met = jnp.int32(4)
    for there, by in ((sp < sp_count - 1, 1), (sp > 0, -1), (z < last, 2), (z > 0, -2)):

        @pl.when(there)
        def _():
            greet(at(sp + by, tp))

        met = met + jnp.where(there, 1, 0)
    pl.semaphore_wait(barrier, met)

    gated = (pre_ref[...].astype(f32) * value_ref[...].astype(f32)).astype(bf16)
    tail[...] = gated[seq - 16 :]
    rim_copy = remote(tail, rim, rim_sem.at[0], rim_sem.at[1], at(sp + 1, tp))

    @pl.when(sp < sp_count - 1)
    def _():
        rim_copy.start()

    expert = lax.broadcasted_iota(jnp.int32, (sp_count, seq), 0)
    spread = jnp.zeros((sp_count, seq), f32)
    for k in range(ids_ref.shape[0]):
        spread = spread + jnp.where(expert == ids_ref[k : k + 1, :], weight_ref[k : k + 1, :], 0.0)
    scales[sp] = spread

    routes = (
        lambda group: (lax.div(group, 2) <= z) & (z < last),
        lambda group: (lax.div(group, 2) >= z) & (z > 0),
    )
    devices = (at(sp + 2, tp), at(sp - 2, tp), at(across, tp), at(sp, sibling), at(sp, opposite))

    def scale_copy(way, group):
        return remote(scales.at[group], scales.at[group], scale_send.at[way], scale_recv.at[group], devices[way])

    def send_scales(group):
        for way in range(2):

            @pl.when(routes[way](group))
            def _():
                scale_copy(way, group).start()

        scale_copy(2, group).start()

    send_scales(sp)
    padded[8:, :] = gated.astype(f32)
    padded[:8, :] = jnp.zeros((8, padded.shape[1]), f32)
    tap_count = taps_ref.shape[0]
    taps = taps_ref[...].astype(f32)

    def mix(count):
        convolved = jnp.zeros((count, padded.shape[1]), f32)
        for k in range(tap_count):
            first = 8 - tap_count + 1 + k
            convolved = convolved + taps[k : k + 1, :] * padded[first : first + count, :]
        mixed[:count, :] = (post_ref[:count, :].astype(f32) * convolved).astype(bf16)

    mix(seq)
    loads[0].wait()

    def rows_of(core):
        return jnp.concatenate(
            [mixed[pl.ds(pl.multiple_of(yy * half + core * rows, rows), rows), :] for yy in range(2)], 0
        )

    def offset_of(p):
        return lax.rem(p + 1, PIECES) * step

    def pair_copy(i):
        if i < 2:
            whose = pl.ds(pl.multiple_of(((1 - y) if i == 0 else y) * rows + step, step), rows - step)
        else:
            whose = pl.ds((3 - i) * rows, step)
        return remote(
            pair_send.at[whose, :], pair_in.at[whose, :], pair_sem.at[0], pair_recv.at[i], at(sp, sibling)
        )

    pair_send[...] = jnp.dot(rows_of(1 - c), out_w[...], preferred_element_type=f32).astype(bf16)
    for i in range(3):
        pair_copy(i).start()

    @pl.when(c == 0)
    def _():
        pair_copy(3).start()

    own_sum[...] = jnp.dot(rows_of(c), out_w[...], preferred_element_type=f32)

    def pair_sum(yy, p):
        piece = pl.ds(pl.multiple_of(yy * rows + offset_of(p), step), step)
        return own_sum[piece, :] + pair_in[piece, :].astype(f32)

    def y_copy(p):
        piece = pl.ds(pl.multiple_of(offset_of(p), step), step)
        return remote(y_send.at[piece, :], y_in.at[piece, :], y_sem.at[0], y_recv.at[p], at(sp, opposite))

    def send_y(p):
        y_send[pl.ds(pl.multiple_of(offset_of(p), step), step), :] = pair_sum(1 - y, p).astype(bf16)
        y_copy(p).start()

    pair_copy(0).wait_recv()
    for p in range(PIECES - 1):
        send_y(p)

    @pl.when(sp > 0)
    def _():
        rim_copy.wait_recv()
        padded[:8, :] = rim[...].astype(f32)[8:]

    mix(step)
    first_rows = jnp.dot(mixed[:step, :], out_w[...], preferred_element_type=f32)

    @pl.when(c == 0)
    def _():
        own_sum[:step, :] = first_rows

    @pl.when(c == 1)
    def _():
        pair_send[:step, :] = first_rows.astype(bf16)
        pair_copy(3).start()

    for i in (2, 3):
        pair_copy(i).wait_recv()
    send_y(PIECES - 1)
    pair_copy(1).wait_recv()

    def height_of(relative):
        inner = jnp.where(relative == 0, 0, jnp.where(relative == 1, -1, relative - 1))
        return z + toward * jnp.where(at_end, relative, inner)

    def wait_scales(group):
        scale_copy(2, group).wait_recv()

    def piece_of(group, yy, p):
        return tokens.at[group, pl.ds(pl.multiple_of((2 * yy + c) * rows + offset_of(p), step), step), :]

    def block_of(group, yy, core):
        return tokens.at[group, pl.ds(pl.multiple_of((2 * yy + core) * rows, rows), rows), :]

    def pass_on(way, group, yy, p):
        piece = piece_of(group, yy, p)
        receive = mate_recv.at[group, yy] if way == 3 else tok_recv.at[group, yy, p]
        return remote(piece, piece, tok_send.at[way], receive, devices[way])

    def sent(way, group_count, row_count):
        rows_sent = tokens.at[pl.ds(0, group_count), pl.ds(0, row_count), :]
        return remote(rows_sent, rows_sent, tok_send.at[way], mate_recv.at[0, 0], devices[way])

    def along_z(group, yy, p):
        for way in range(2):

            @pl.when(routes[way](group))
            def _():
                pass_on(way, group, yy, p).start()

    for p in range(PIECES):
        y_copy(p).wait_recv()
        piece = pl.ds(pl.multiple_of(offset_of(p), step), step)
        residual = (
            stream_ref[piece, :].astype(f32) + (pair_sum(y, p) + y_in[piece, :].astype(f32))
        ).astype(bf16)
        resid[piece, :] = residual
        tokens[sp, pl.ds(pl.multiple_of(tp * rows + offset_of(p), step), step), :] = scaled_norm(
            residual.astype(f32), gain_ref[...].reshape(1, width)
        ).astype(bf16)
        pass_on(4, sp, y, p).start()
        along_z(sp, y, p)
        pass_on(2, sp, y, p).start()
        pass_on(3, sp, y, p).start()

    for load in loads[1:]:
        load.wait()

    def wait_piece(group, yy, p):
        pass_on(2, group, yy, p).wait_recv()

    def wait_mate(group, yy):
        block = block_of(group, yy, 1 - c)
        remote(block, block, tok_send.at[3], mate_recv.at[group, yy], at(sp, sibling)).wait_recv()

    def block_at(code):
        relative, second, p = lax.div(code, 2 * PIECES), lax.rem(lax.div(code, PIECES), 2), lax.rem(code, PIECES)
        return relative, height_of(relative), jnp.where(second == 0, y, 1 - y), p

    def take(code):
        relative, height, yy, p = block_at(code)
        group = 2 * height + x

        @pl.when((relative > 0) & (lax.rem(code, 2 * PIECES) == 0))
        def _():
            wait_scales(group)
            send_scales(group)

        wait_piece(group, yy, p)

        @pl.when((relative > 0) | at_end)
        def _():
            along_z(group, yy, p)

        pass_on(3, group, yy, p).start()

        @pl.when(relative > 0)
        def _():
            pass_on(2, group, yy, p).start()

    def take_across(code):
        _, height, yy, p = block_at(code)
        group = 2 * height + 1 - x

        @pl.when(lax.rem(code, 2 * PIECES) == 0)
        def _():
            wait_scales(group)

        wait_piece(group, yy, p)
        pass_on(3, group, yy, p).start()

    def pass_held(code):
        p = lax.rem(code, PIECES)

        @pl.when(code < PIECES)
        def _():
            pass_on(2, sp, 1 - y, p).start()

        @pl.when(code >= PIECES)
        def _():
            along_z(sp, 1 - y, p)

    def tile_at(tile):
        height = height_of(lax.div(tile, 4))
        side = jnp.where(lax.rem(lax.div(tile, 2), 2) == 0, x, 1 - x)
        return height, 2 * height + side, jnp.where(lax.rem(tile, 2) == 0, y, 1 - y)

    def tile_rows(yy):
        return pl.ds(pl.multiple_of(yy * half, half), half)

    def share(way, group, yy):
        whose = tp if way < 2 else opposite
        block = hidden.at[group, whose, tile_rows(yy), :]
        receive = mate_hid_recv.at[group, yy] if way else hid_recv.at[group, yy]
        return remote(block, block, hid_send.at[way], receive, at(sp, sibling if way else opposite))

    def gated_units(tile):
        _, group, yy = tile_at(tile)
        wait_mate(group, yy)
        inputs = tokens[group, tile_rows(yy), :]
        span = min(256, units)
        for start in range(0, units, span):
            gate_pre = jnp.dot(inputs, gate_w[:, start : start + span], preferred_element_type=f32)
            up_pre = jnp.dot(inputs, up_w[:, start : start + span], preferred_element_type=f32)
            hidden[group, tp, tile_rows(yy), start : start + span] = clamped_units(gate_pre, up_pre).astype(bf16)
        share(0, group, yy).start()
        share(1, group, yy).start()

    def relay_units(tile):
        _, group, yy = tile_at(tile)
        share(0, group, yy).wait_recv()
        share(2, group, yy).start()

    def chain_copy(group, yy):
        rising = lax.div(group, 2) > z
        return remote(
            part.at[group, tile_rows(yy), :],
            chain_in.at[jnp.where(rising, 0, 1), group, tile_rows(yy), :],
            chain_send.at[0],
            chain_recv.at[group, yy],
            at(sp + jnp.where(rising, 2, -2), tp),
        )

    def wait_chain(sides, group, yy):
        tiles = chain_in.at[pl.ds(0, sides), group, tile_rows(yy), :]
        remote(tiles, tiles, chain_send.at[0], chain_recv.at[group, yy], at(sp, sibling)).wait_recv()

    diagonal = lax.broadcasted_iota(jnp.int32, (half, half), 0) == lax.broadcasted_iota(jnp.int32, (half, half), 1)

    def project_down(tile):
        height, group, yy = tile_at(tile)
        both = hidden.at[group, pl.ds(0, 2), tile_rows(yy), :]
        remote(both, both, hid_send.at[1], mate_hid_recv.at[group, yy], at(sp, sibling)).wait_recv()
        own_rows = tile_rows(yy)
        out = jnp.dot(hidden[group, 0, own_rows, :], down_w[:units, :], preferred_element_type=f32)
        for k in range(1, 4):
            out = out + jnp.dot(
                hidden[group, k, own_rows, :], down_w[k * units : (k + 1) * units, :], preferred_element_type=f32
            )
        weight = scales[group, :, tile_rows(yy)]
        mine = lax.broadcasted_iota(jnp.int32, weight.shape, 0) == sp
        weight = jnp.sum(jnp.where(mine, weight, 0.0), axis=0, keepdims=True)
        weight = jnp.sum(jnp.where(diagonal, weight, 0.0), axis=1, keepdims=True)
        part[group, own_rows, :] = (out.astype(bf16).astype(f32) * weight).astype(bf16)

        @pl.when(((height > z) & (z == 0)) | ((height < z) & (z == last)))
        def _():
            chain_copy(group, yy).start()

    def x_copy(group, yy):
        return remote(
            part.at[group, tile_rows(yy), :], x_in.at[tile_rows(yy), :], x_send.at[0], x_recv.at[yy], at(across, tp)
        )

    def hand_over(to):
        return remote(
            final.at[pl.ds(to * rows, rows), :], columns.at[tp], fin_send.at[0], fin_recv.at[tp], at(sp, to)
        )

    def toward_home(tile):
        height, group, yy = tile_at(tile)
        own_rows = tile_rows(yy)
        total[...] = part[group, own_rows, :].astype(f32)
        both_sides = (height == z) & jnp.logical_not(at_end)

        @pl.when(both_sides)
        def _():
            wait_chain(2, group, yy)

        @pl.when(jnp.logical_not(both_sides))
        def _():
            wait_chain(1, group, yy)

        for side, comes in enumerate(((height >= z) & (z > 0), (height <= z) & (z < last))):

            @pl.when(comes)
            def _():
                total[...] = total[...] + chain_in[side, group, own_rows, :].astype(f32)

        @pl.when(group != sp)
        def _():
            part[group, own_rows, :] = total[...].astype(bf16)

            @pl.when(height != z)
            def _():
                chain_copy(group, yy).start()

            @pl.when(height == z)
            def _():
                x_copy(group, yy).start()

        @pl.when(group == sp)
        def _():
            x_copy(group, yy).wait_recv()
            final[own_rows, :] = (total[...] + x_in[own_rows, :].astype(f32)).astype(bf16)
            for to in range(4):

                @pl.when((tp != to) & (yy == to // 2))
                def _():
                    hand_over(to).start()

    acts = (take, take_across, pass_held, gated_units, relay_units, project_down, toward_home)

    def four_events(position, carry):
        word = pick(at_end, plans, position)

        def event(i, carry):
            code = lax.shift_right_logical(word, 8 * i) & 255
            kind, rest = lax.div(code, 32), lax.rem(code, 32)
            for j, act in enumerate(acts):

                @pl.when(kind == j)
                def _():
                    act(rest)

            return carry

        return lax.fori_loop(0, 4, event, carry)

    plans = [words_of(plan) for plan in (end_plan, middle_plan)]
    lax.fori_loop(0, max(len(plan) for plan in plans), four_events, 0)

    columns[tp] = final[pl.ds(pl.multiple_of(tp * rows, rows), rows), :]
    for by in (1, 2, 3):
        whose = lax.rem(tp + by, 4)
        remote(
            final.at[pl.ds(0, rows), :], columns.at[whose], fin_send.at[0], fin_recv.at[whose], at(sp, sibling)
        ).wait_recv()
    combined = jnp.concatenate([columns[k] for k in range(4)], 1).astype(f32)
    result_ref[...] = (
        resid[...].astype(f32) + scaled_norm(combined, post_gain_ref[...].reshape(1, width))
    ).astype(bf16)

    @pl.when(sp < sp_count - 1)
    def _():
        rim_copy.wait_send()

    remote(pair_send, pair_in, pair_sem.at[0], pair_recv.at[0], at(sp, sibling)).wait_send()
    remote(y_send, y_in, y_sem.at[0], y_recv.at[0], at(sp, opposite)).wait_send()
    sent(4, 1, rows).wait_send()
    sent(3, heights, seq).wait_send()
    sent(2, heights, half).wait_send()

    def scales_sent(way, group_count):
        blocks = scales.at[pl.ds(0, group_count)]
        remote(blocks, blocks, scale_send.at[way], scale_recv.at[0], devices[way]).wait_send()

    scales_sent(2, heights)
    for count in range(1, heights):
        for way, its in enumerate((z == count - 1, z == heights - count)):

            @pl.when(its)
            def _():
                sent(way, count, half).wait_send()
                scales_sent(way, count)

    for way in range(3):
        tiles = hidden.at[:, 0]
        receive = mate_hid_recv.at[0, 0] if way else hid_recv.at[0, 0]
        remote(tiles, tiles, hid_send.at[way], receive, at(sp, sibling)).wait_send()
    chained = part.at[pl.ds(0, sp_count - 2)]
    remote(chained, chained, chain_send.at[0], chain_recv.at[0, 0], at(sp, sibling)).wait_send()
    remote(part.at[0], x_in, x_send.at[0], x_recv.at[0], at(across, tp)).wait_send()
    handed = final.at[pl.ds(0, 3 * rows), :]
    remote(handed, handed, fin_send.at[0], fin_recv.at[0], at(sp, sibling)).wait_send()


def dense_layer(
    stream_in,
    pre_gate,
    value_in,
    post_gate,
    conv_taps,
    out_weight,
    route_ids,
    route_weight,
    ffn_gain,
    post_gain,
    gate_proj,
    up_proj,
    down_proj,
):
    sp_count = lax.axis_size("sp")
    rows, width = stream_in.shape
    seq, channels = pre_gate.shape
    units = gate_proj.shape[2]
    cols = down_proj.shape[2]
    bf16, f32 = jnp.bfloat16, jnp.float32
    dma = pltpu.SemaphoreType.DMA
    scratch = [
        pltpu.VMEM(out_weight.shape, bf16),
        pltpu.VMEM(gate_proj.shape[1:], bf16),
        pltpu.VMEM(up_proj.shape[1:], bf16),
        pltpu.VMEM(down_proj.shape[1:], bf16),
        pltpu.VMEM((16, channels), bf16),
        pltpu.VMEM((16, channels), bf16),
        pltpu.VMEM((seq + 8, channels), f32),
        pltpu.VMEM((seq, channels), bf16),
        pltpu.VMEM((2 * rows, width), bf16),
        pltpu.VMEM((2 * rows, width), bf16),
        pltpu.VMEM((2 * rows, width), f32),
        pltpu.VMEM((rows, width), bf16),
        pltpu.VMEM((rows, width), bf16),
        pltpu.VMEM((rows, width), bf16),
        pltpu.VMEM((sp_count, sp_count, seq), f32),
        pltpu.VMEM((sp_count, seq, width), bf16),
        pltpu.VMEM((sp_count, 4, seq, units), bf16),
        pltpu.VMEM((sp_count, seq, cols), bf16),
        pltpu.VMEM((2, sp_count, seq, cols), bf16),
        pltpu.VMEM((seq, cols), bf16),
        pltpu.VMEM((2 * rows, cols), f32),
        pltpu.VMEM((seq, cols), bf16),
        pltpu.VMEM((4, rows, cols), bf16),
        dma((4,)),
        dma((2,)),
        dma((1,)),
        dma((4,)),
        dma((1,)),
        dma((PIECES,)),
        dma((3,)),
        dma((sp_count,)),
        dma((5,)),
        dma((sp_count, 2, PIECES)),
        dma((sp_count, 2)),
        dma((3,)),
        dma((sp_count, 2)),
        dma((sp_count, 2)),
        dma((1,)),
        dma((sp_count, 2)),
        dma((1,)),
        dma((2,)),
        dma((1,)),
        dma((4,)),
    ]
    vmem = pl.BlockSpec(memory_space=pltpu.VMEM)
    anywhere = pl.BlockSpec(memory_space=pl.ANY)
    return pl.pallas_call(
        functools.partial(layer_kernel, sp_count),
        out_shape=jax.ShapeDtypeStruct((rows, width), bf16),
        in_specs=[vmem] * 9 + [anywhere] * 4,
        out_specs=vmem,
        scratch_shapes=scratch,
        compiler_params=pltpu.CompilerParams(
            collective_id=0, has_side_effects=True, vmem_limit_bytes=58 * 1024 * 1024
        ),
    )(
        stream_in,
        pre_gate,
        value_in,
        post_gate,
        conv_taps,
        route_ids.T,
        route_weight.T,
        ffn_gain,
        post_gain,
        out_weight,
        gate_proj,
        up_proj,
        down_proj,
    )


def local(
    stream_in,
    pre_gate,
    value_in,
    post_gate,
    conv_taps,
    out_weight,
    route_ids,
    route_weight,
    ffn_gain,
    post_gain,
    gate_proj,
    up_proj,
    down_proj,
):
    sp_count = lax.axis_size("sp")
    tp_count = lax.axis_size("tp")
    seq_rows = pre_gate.shape[0]
    own_rows = seq_rows // tp_count
    top_count = route_ids.shape[1]
    slots_each = 2 * own_rows * top_count // sp_count
    if tp_count == 4 and sp_count == PLANNED_GROUPS and slots_each >= own_rows:
        return dense_layer(
            stream_in, pre_gate, value_in, post_gate, conv_taps, out_weight, route_ids, route_weight,
            ffn_gain, post_gain, gate_proj, up_proj, down_proj,
        )
    tap_count = conv_taps.shape[0]
    gated_input = (pre_gate.astype(jnp.float32) * value_in.astype(jnp.float32)).astype(jnp.bfloat16)
    rim_rows = passed_along(gated_input[seq_rows - tap_count + 1 :], "sp", 1)
    padded = jnp.concatenate([rim_rows, gated_input], 0).astype(jnp.float32)
    convolved = jnp.zeros(gated_input.shape, jnp.float32)
    for tap_index in range(tap_count):
        convolved = (
            convolved
            + conv_taps[tap_index].astype(jnp.float32)[None, :]
            * padded[tap_index : tap_index + seq_rows]
        )
    mixer_out = (post_gate.astype(jnp.float32) * convolved).astype(jnp.bfloat16)
    weight_rows = mixer_out
    projected = lax.psum_scatter(
        jnp.dot(weight_rows, out_weight, preferred_element_type=jnp.float32),
        "tp",
        scatter_dimension=0,
        tiled=True,
    )
    residual = (stream_in.astype(jnp.float32) + projected).astype(jnp.bfloat16)
    normed = scaled_norm(residual.astype(jnp.float32), ffn_gain).astype(jnp.bfloat16)
    slot_rank = block_ranks(route_ids, sp_count, own_rows)
    block_of = (jnp.arange(seq_rows, dtype=jnp.int32) // own_rows)[:, None]
    tp_index = lax.axis_index("tp")
    own_ids = lax.dynamic_slice_in_dim(route_ids, tp_index * own_rows, own_rows, 0)
    own_rank = lax.dynamic_slice_in_dim(slot_rank, tp_index * own_rows, own_rows, 0)
    own_slot = own_ids * slots_each + own_rank
    picker = slot_picker(own_slot, sp_count * slots_each)
    outgoing = jnp.dot(picker, normed, preferred_element_type=jnp.float32).astype(jnp.bfloat16)
    arrived = lax.all_to_all(outgoing, "sp", split_axis=0, concat_axis=0, tiled=True)
    portion = lax.all_gather(arrived, "tp", axis=0, tiled=True)
    gate_pre = jnp.dot(portion, gate_proj[0], preferred_element_type=jnp.float32)
    up_pre = jnp.dot(portion, up_proj[0], preferred_element_type=jnp.float32)
    hidden = clamped_units(gate_pre, up_pre).astype(jnp.bfloat16)
    weight_rows = down_proj[0]
    column_out = jnp.dot(
        lax.all_gather(hidden, "tp", axis=1, tiled=True),
        weight_rows,
        preferred_element_type=jnp.float32,
    ).astype(jnp.bfloat16)
    column_width = column_out.shape[1]
    returned = lax.all_to_all(
        column_out.reshape(tp_count, sp_count, slots_each, column_width),
        "sp",
        split_axis=1,
        concat_axis=1,
        tiled=True,
    )
    home_index = (block_of * sp_count + route_ids) * slots_each + slot_rank
    gathered_out = jnp.take(returned.reshape(-1, column_width), home_index.reshape(-1), axis=0)
    gathered_out = gathered_out.astype(jnp.float32).reshape(seq_rows, top_count, column_width)
    combined_cols = jnp.sum(gathered_out * route_weight[:, :, None], axis=1).astype(jnp.bfloat16)
    combined = lax.all_to_all(combined_cols, "tp", split_axis=0, concat_axis=1, tiled=True)
    layer_out = residual.astype(jnp.float32) + scaled_norm(combined.astype(jnp.float32), post_gain)
    return layer_out.astype(jnp.bfloat16)


def solution(mesh):
    placed = (
        P(("sp", "tp"), None),
        P("sp", "tp"),
        P("sp", "tp"),
        P("sp", "tp"),
        P(None, "tp"),
        P("tp", None),
        P("sp", None),
        P("sp", None),
        P(),
        P(),
        P("sp", None, "tp"),
        P("sp", None, "tp"),
        P("sp", None, "tp"),
    )
    return jax.shard_map(
        local, mesh=mesh, in_specs=placed, out_specs=P(("sp", "tp"), None), check_vma=False
    )
```

```python
import functools

import jax
import jax.numpy as jnp
from jax import lax
from jax.experimental import pallas as pl
from jax.experimental.pallas import tpu as pltpu
from jax.sharding import PartitionSpec as P

clamp_limit = 7.0
sigmoid_scale = 1.702
epsilon = 1e-06


def passed_along(array, axis, by):
    count = lax.axis_size(axis)
    pairs = [(i, i + by) for i in range(count) if 0 <= i + by < count]
    return lax.ppermute(array, axis, pairs)


def clamped_units(gate_pre, up_pre):
    gate_cut = jnp.minimum(gate_pre, clamp_limit)
    up_cut = jnp.clip(up_pre, -clamp_limit, clamp_limit)
    return (up_cut + 1.0) * (gate_cut * jax.nn.sigmoid(sigmoid_scale * gate_cut))


def scaled_norm(values, gain):
    return (
        values
        * lax.rsqrt(jnp.mean(values * values, axis=-1, keepdims=True) + epsilon)
        * gain.astype(jnp.float32)
    )


def block_ranks(route_rows, experts, block_rows):
    flattened = route_rows.reshape(-1)
    entries = flattened.shape[0]
    span_width = block_rows * route_rows.shape[1]
    onehot = (flattened[:, None] == jnp.arange(experts, dtype=jnp.int32)[None, :]).astype(jnp.int32)
    blocked = onehot.reshape(entries // span_width, span_width, experts)
    before = jnp.cumsum(blocked, axis=1) - blocked
    return jnp.sum(before * blocked, axis=2).reshape(route_rows.shape)


def slot_picker(slot_index, table_size):
    matches = slot_index[None, :, :] == jnp.arange(table_size, dtype=jnp.int32)[:, None, None]
    return jnp.any(matches, axis=2).astype(jnp.bfloat16)


PIECES = 4
PLANNED_GROUPS = 8
end_plan = (
    8, 96, 10, 5, 11, 9, 4, 7, 100, 16, 6, 18, 19, 97, 42, 41, 17, 40, 43, 102,
    24, 104, 27, 25, 26, 59, 50, 108, 31, 56, 29, 57, 30, 28, 58, 109, 48, 51, 49, 12,
    141, 106, 14, 173, 218, 110, 63, 60, 133, 62, 135, 13, 219, 140, 15, 61, 20, 22, 111, 101,
    172, 216, 165, 139, 129, 23, 21, 45, 217, 44, 143, 66, 65, 175, 105, 52, 47, 54, 35, 137,
    223, 33, 46, 67, 142, 64, 55, 128, 53, 32, 222, 174, 221, 107, 103, 161, 34, 171, 215, 167,
    214, 98, 207, 132, 39, 206, 169, 220, 138, 36, 136, 38, 37, 211, 210, 170, 213, 99, 203, 134,
    212, 168, 166, 204, 202, 205, 209, 131, 163, 199, 164, 198, 130, 208, 200, 201, 162, 197, 160, 195,
    196, 194, 193, 192,
)
middle_plan = (
    16, 8, 4, 17, 96, 10, 11, 18, 6, 9, 19, 13, 100, 24, 27, 5, 7, 97, 25, 15,
    26, 14, 29, 12, 35, 34, 108, 42, 40, 31, 41, 30, 101, 28, 68, 133, 128, 70, 129, 69,
    43, 109, 32, 104, 71, 102, 132, 59, 22, 33, 57, 161, 98, 160, 20, 58, 141, 21, 51, 56,
    48, 23, 140, 49, 65, 50, 173, 110, 172, 62, 61, 64, 105, 66, 67, 218, 47, 131, 63, 46,
    44, 60, 143, 45, 111, 219, 106, 103, 175, 54, 55, 53, 52, 165, 217, 135, 216, 164, 142, 223,
    107, 222, 174, 139, 167, 202, 137, 36, 38, 221, 37, 39, 207, 171, 215, 136, 134, 99, 206, 203,
    214, 166, 163, 220, 199, 138, 198, 205, 168, 170, 200, 169, 211, 213, 212, 210, 204, 130, 162, 201,
    197, 196, 209, 194, 208, 195, 193, 192,
)
x_first = (
    ((1, 0), (1, 1), (2, 0),),
    ((2, 0), (2, 1),),
)

def comes_along_z(x_first_end, x_first_middle):
    near, far = [0, 0], [0, 0]
    for tile in range(16):
        height, across, second = tile // 4, tile // 2 % 2, tile % 2
        if height == 0 and not (across and (1, second) in x_first_middle):
            far[0] |= 1 << tile
        if not (across and (height or 1, second) in x_first_end) and height != 1:
            near[1] |= 1 << tile
        if height < 2 and not (across and ((2, 3)[height], second) in x_first_middle):
            far[1] |= 1 << tile
    return near, far


def words_of(plan):
    codes = list(plan)
    codes += [255] * (-len(codes) % 4)
    words = [sum(code << (8 * i) for i, code in enumerate(codes[at : at + 4])) for at in range(0, len(codes), 4)]
    return [word - (1 << 32) if word >> 31 else word for word in words]


def pick(at_end, tables, position):
    value = jnp.int32(-1)
    for i, table in enumerate(tables):
        chosen = jnp.int32(-1)
        for j, word in enumerate(table):
            chosen = jnp.where(position == j, word, chosen)
        value = jnp.where(at_end == (i == 0), chosen, value)
    return value


def layer_kernel(
    sp_count,
    stream_hbm,
    pre_hbm,
    value_hbm,
    post_hbm,
    taps_hbm,
    ids_hbm,
    weight_hbm,
    gain_hbm,
    post_gain_hbm,
    out_hbm,
    gate_hbm,
    up_hbm,
    down_hbm,
    result_ref,
    stream_ref,
    pre_ref,
    value_ref,
    post_ref,
    taps_ref,
    ids_ref,
    weight_ref,
    gain_ref,
    post_gain_ref,
    out_w,
    gate_w,
    up_w,
    down_w,
    tail,
    rim,
    padded,
    mixed,
    pair_send,
    pair_in,
    own_sum,
    y_send,
    y_in,
    resid,
    scales,
    tokens,
    hidden,
    part,
    chain_in,
    x_in,
    total,
    final,
    columns,
    load_sem,
    rim_sem,
    pair_sem,
    pair_recv,
    y_sem,
    y_recv,
    scale_send,
    scale_recv,
    tok_send,
    tok_recv,
    mate_recv,
    hid_send,
    hid_recv,
    mate_hid_recv,
    chain_send,
    chain_recv,
    x_send,
    x_recv,
    fin_send,
    fin_recv,
):
    f32, bf16 = jnp.float32, jnp.bfloat16
    heights = sp_count // 2
    last = heights - 1
    sp = lax.axis_index("sp")
    tp = lax.axis_index("tp")
    z, x = lax.div(sp, 2), lax.rem(sp, 2)
    y, c = lax.div(tp, 2), lax.rem(tp, 2)
    across, sibling = sp + 1 - 2 * x, tp + 1 - 2 * c
    opposite = lax.rem(tp + 2, 4)
    rows, width = stream_ref.shape
    seq = 4 * rows
    half = 2 * rows
    step = rows // PIECES
    units = gate_w.shape[1]
    at_end = (z == 0) | (z == last)
    toward = jnp.where(2 * z < heights, 1, -1)

    def at(sp_to, tp_to):
        return {"sp": sp_to, "tp": tp_to}

    def remote(source, target, send, receive, device):
        return pltpu.make_async_remote_copy(
            src_ref=source,
            dst_ref=target,
            send_sem=send,
            recv_sem=receive,
            device_id=device,
            device_id_type=pl.DeviceIdType.MESH,
        )

    sources = dict(
        pre=(pre_hbm, pre_ref),
        value=(value_hbm, value_ref),
        ids=(ids_hbm, ids_ref),
        weight=(weight_hbm, weight_ref),
        taps=(taps_hbm, taps_ref),
        post=(post_hbm, post_ref),
        out=(out_hbm, out_w),
        stream=(stream_hbm, stream_ref),
        gain=(gain_hbm, gain_ref),
        gate=(gate_hbm.at[0], gate_w),
        up=(up_hbm.at[0], up_w),
        down=(down_hbm.at[0], down_w),
        post_gain=(post_gain_hbm, post_gain_ref),
    )
    loads = {
        name: pltpu.make_async_copy(source, target, load_sem.at[i])
        for i, (name, (source, target)) in enumerate(sources.items())
    }
    for load in loads.values():
        load.start()

    def loaded(*wanted):
        for name in wanted:
            loads[name].wait()

    barrier = pltpu.get_barrier_semaphore()

    def greet(partner):
        pl.semaphore_signal(barrier, inc=1, device_id=partner, device_id_type=pl.DeviceIdType.MESH)

    for partner in (at(across, tp), at(sp, sibling), at(sp, opposite), at(sp, 3 - tp)):
        greet(partner)
    met = jnp.int32(4)
    for there, by in ((sp < sp_count - 1, 1), (sp > 0, -1), (z < last, 2), (z > 0, -2)):

        @pl.when(there)
        def _():
            greet(at(sp + by, tp))

        met = met + jnp.where(there, 1, 0)
    pl.semaphore_wait(barrier, met)

    loaded("pre", "value")
    gated = (pre_ref[...].astype(f32) * value_ref[...].astype(f32)).astype(bf16)
    tail[...] = gated[seq - 16 :]
    rim_copy = remote(tail, rim, rim_sem.at[0], rim_sem.at[1], at(sp + 1, tp))

    @pl.when(sp < sp_count - 1)
    def _():
        rim_copy.start()

    loaded("ids", "weight")
    expert = lax.broadcasted_iota(jnp.int32, (sp_count, seq), 0)
    spread = jnp.zeros((sp_count, seq), f32)
    for k in range(ids_ref.shape[0]):
        spread = spread + jnp.where(expert == ids_ref[k : k + 1, :], weight_ref[k : k + 1, :], 0.0)
    scales[sp] = spread

    routes = (
        lambda group: (lax.div(group, 2) <= z) & (z < last),
        lambda group: (lax.div(group, 2) >= z) & (z > 0),
    )
    devices = (at(sp + 2, tp), at(sp - 2, tp), at(across, tp), at(sp, sibling), at(sp, opposite))

    def scale_copy(way, group):
        return remote(scales.at[group], scales.at[group], scale_send.at[way], scale_recv.at[group], devices[way])

    def send_scales(group):
        for way in range(2):

            @pl.when(routes[way](group))
            def _():
                scale_copy(way, group).start()

        scale_copy(2, group).start()

    send_scales(sp)
    padded[8:, :] = gated.astype(f32)
    padded[:8, :] = jnp.zeros((8, padded.shape[1]), f32)
    loaded("taps", "post")
    tap_count = taps_ref.shape[0]
    taps = taps_ref[...].astype(f32)

    def mix(count):
        convolved = jnp.zeros((count, padded.shape[1]), f32)
        for k in range(tap_count):
            first = 8 - tap_count + 1 + k
            convolved = convolved + taps[k : k + 1, :] * padded[first : first + count, :]
        mixed[:count, :] = (post_ref[:count, :].astype(f32) * convolved).astype(bf16)

    mix(seq)
    loaded("out")

    def rows_of(core):
        return jnp.concatenate(
            [mixed[pl.ds(pl.multiple_of(yy * half + core * rows, rows), rows), :] for yy in range(2)], 0
        )

    def offset_of(p):
        return lax.rem(p + 1, PIECES) * step

    def pair_copy(i):
        if i < 2:
            whose = pl.ds(pl.multiple_of(((1 - y) if i == 0 else y) * rows + step, step), rows - step)
        else:
            whose = pl.ds((3 - i) * rows, step)
        return remote(
            pair_send.at[whose, :], pair_in.at[whose, :], pair_sem.at[0], pair_recv.at[i], at(sp, sibling)
        )

    pair_send[...] = jnp.dot(rows_of(1 - c), out_w[...], preferred_element_type=f32).astype(bf16)
    for i in range(3):
        pair_copy(i).start()

    @pl.when(c == 0)
    def _():
        pair_copy(3).start()

    own_sum[...] = jnp.dot(rows_of(c), out_w[...], preferred_element_type=f32)

    def pair_sum(yy, p):
        piece = pl.ds(pl.multiple_of(yy * rows + offset_of(p), step), step)
        return own_sum[piece, :] + pair_in[piece, :].astype(f32)

    def y_copy(p):
        piece = pl.ds(pl.multiple_of(offset_of(p), step), step)
        return remote(y_send.at[piece, :], y_in.at[piece, :], y_sem.at[0], y_recv.at[p], at(sp, opposite))

    def send_y(p):
        y_send[pl.ds(pl.multiple_of(offset_of(p), step), step), :] = pair_sum(1 - y, p).astype(bf16)
        y_copy(p).start()

    pair_copy(0).wait_recv()
    for p in range(PIECES - 1):
        send_y(p)

    @pl.when(sp > 0)
    def _():
        rim_copy.wait_recv()
        padded[:8, :] = rim[...].astype(f32)[8:]

    mix(step)
    first_rows = jnp.dot(mixed[:step, :], out_w[...], preferred_element_type=f32)

    @pl.when(c == 0)
    def _():
        own_sum[:step, :] = first_rows

    @pl.when(c == 1)
    def _():
        pair_send[:step, :] = first_rows.astype(bf16)
        pair_copy(3).start()

    for i in (2, 3):
        pair_copy(i).wait_recv()
    send_y(PIECES - 1)
    pair_copy(1).wait_recv()
    loaded("stream", "gain")

    def height_of(relative):
        inner = jnp.where(relative == 0, 0, jnp.where(relative == 1, -1, relative - 1))
        return z + toward * jnp.where(at_end, relative, inner)

    def wait_scales(group):
        scale_copy(2, group).wait_recv()

    def piece_of(group, yy, p):
        return tokens.at[group, pl.ds(pl.multiple_of((2 * yy + c) * rows + offset_of(p), step), step), :]

    def block_of(group, yy, core):
        return tokens.at[group, pl.ds(pl.multiple_of((2 * yy + core) * rows, rows), rows), :]

    def pass_on(way, group, yy, p):
        piece = piece_of(group, yy, p)
        receive = mate_recv.at[group, yy] if way == 3 else tok_recv.at[group, yy, p]
        return remote(piece, piece, tok_send.at[way], receive, devices[way])

    def sent(way, group_count, row_count):
        rows_sent = tokens.at[pl.ds(0, group_count), pl.ds(0, row_count), :]
        return remote(rows_sent, rows_sent, tok_send.at[way], mate_recv.at[0, 0], devices[way])

    def along_z(group, yy, p):
        for way in range(2):

            @pl.when(routes[way](group))
            def _():
                pass_on(way, group, yy, p).start()

    for p in range(PIECES):
        y_copy(p).wait_recv()
        piece = pl.ds(pl.multiple_of(offset_of(p), step), step)
        residual = (
            stream_ref[piece, :].astype(f32) + (pair_sum(y, p) + y_in[piece, :].astype(f32))
        ).astype(bf16)
        resid[piece, :] = residual
        tokens[sp, pl.ds(pl.multiple_of(tp * rows + offset_of(p), step), step), :] = scaled_norm(
            residual.astype(f32), gain_ref[...].reshape(1, width)
        ).astype(bf16)
        pass_on(4, sp, y, p).start()
        along_z(sp, y, p)
        pass_on(2, sp, y, p).start()
        pass_on(3, sp, y, p).start()

    loaded("gate", "up", "down")

    def wait_piece(group, yy, p):
        pass_on(2, group, yy, p).wait_recv()

    def wait_mate(group, yy):
        block = block_of(group, yy, 1 - c)
        remote(block, block, tok_send.at[3], mate_recv.at[group, yy], at(sp, sibling)).wait_recv()

    def block_at(code):
        relative, second, p = lax.div(code, 2 * PIECES), lax.rem(lax.div(code, PIECES), 2), lax.rem(code, PIECES)
        return relative, height_of(relative), jnp.where(second == 0, y, 1 - y), p

    def take(code):
        relative, height, yy, p = block_at(code)
        group = 2 * height + x

        @pl.when((relative > 0) & (lax.rem(code, 2 * PIECES) == 0))
        def _():
            wait_scales(group)
            send_scales(group)

        wait_piece(group, yy, p)

        @pl.when((relative > 0) | at_end)
        def _():
            along_z(group, yy, p)

        pass_on(3, group, yy, p).start()

        @pl.when(relative > 0)
        def _():
            pass_on(2, group, yy, p).start()

    def take_across(code):
        _, height, yy, p = block_at(code)
        group = 2 * height + 1 - x

        @pl.when(lax.rem(code, 2 * PIECES) == 0)
        def _():
            wait_scales(group)

        wait_piece(group, yy, p)
        pass_on(3, group, yy, p).start()

    def pass_held(code):
        p = lax.rem(code, PIECES)

        @pl.when(code < PIECES)
        def _():
            pass_on(2, sp, 1 - y, p).start()

        @pl.when(code >= PIECES)
        def _():
            along_z(sp, 1 - y, p)

    def tile_at(tile):
        height = height_of(lax.div(tile, 4))
        side = jnp.where(lax.rem(lax.div(tile, 2), 2) == 0, x, 1 - x)
        return height, 2 * height + side, jnp.where(lax.rem(tile, 2) == 0, y, 1 - y)

    def tile_rows(yy):
        return pl.ds(pl.multiple_of(yy * half, half), half)

    def share(way, group, yy):
        whose = tp if way < 2 else opposite
        block = hidden.at[group, whose, tile_rows(yy), :]
        receive = mate_hid_recv.at[group, yy] if way else hid_recv.at[group, yy]
        return remote(block, block, hid_send.at[way], receive, at(sp, sibling if way else opposite))

    def gated_units(tile):
        _, group, yy = tile_at(tile)
        wait_mate(group, yy)
        inputs = tokens[group, tile_rows(yy), :]
        span = min(256, units)
        for start in range(0, units, span):
            gate_pre = jnp.dot(inputs, gate_w[:, start : start + span], preferred_element_type=f32)
            up_pre = jnp.dot(inputs, up_w[:, start : start + span], preferred_element_type=f32)
            hidden[group, tp, tile_rows(yy), start : start + span] = clamped_units(gate_pre, up_pre).astype(bf16)
        share(0, group, yy).start()
        share(1, group, yy).start()

    def relay_units(tile):
        _, group, yy = tile_at(tile)
        share(0, group, yy).wait_recv()
        share(2, group, yy).start()

    def own_half(yy, h):
        return pl.ds(pl.multiple_of(yy * half + h * rows, rows), rows)

    def chain_copy(group, yy, h):
        rising = lax.div(group, 2) > z
        return remote(
            part.at[group, own_half(yy, h), :],
            chain_in.at[jnp.where(at_end, 0, 1), group, own_half(yy, h), :],
            chain_send.at[0],
            chain_recv.at[group, yy, h],
            at(sp + jnp.where(rising, 2, -2), tp),
        )

    def wait_chain(sides, group, yy, h):
        tiles = chain_in.at[pl.ds(0, sides), group, own_half(yy, h), :]
        remote(tiles, tiles, chain_send.at[0], chain_recv.at[group, yy, h], at(sp, sibling)).wait_recv()

    diagonal = lax.broadcasted_iota(jnp.int32, (half, half), 0) == lax.broadcasted_iota(jnp.int32, (half, half), 1)

    def project_down(tile):
        _, group, yy = tile_at(tile)
        both = hidden.at[group, pl.ds(0, 2), tile_rows(yy), :]
        remote(both, both, hid_send.at[1], mate_hid_recv.at[group, yy], at(sp, sibling)).wait_recv()
        own_rows = tile_rows(yy)
        out = jnp.dot(hidden[group, 0, own_rows, :], down_w[:units, :], preferred_element_type=f32)
        for k in range(1, 4):
            out = out + jnp.dot(
                hidden[group, k, own_rows, :], down_w[k * units : (k + 1) * units, :], preferred_element_type=f32
            )
        weight = scales[group, :, tile_rows(yy)]
        mine = lax.broadcasted_iota(jnp.int32, weight.shape, 0) == sp
        weight = jnp.sum(jnp.where(mine, weight, 0.0), axis=0, keepdims=True)
        weight = jnp.sum(jnp.where(diagonal, weight, 0.0), axis=1, keepdims=True)
        part[group, own_rows, :] = (out.astype(bf16).astype(f32) * weight).astype(bf16)

    def x_copy(group, yy, h):
        height = lax.div(group, 2)
        return remote(
            part.at[group, own_half(yy, h), :],
            x_in.at[height, own_half(yy, h), :],
            x_send.at[0],
            x_recv.at[height, yy, h],
            at(across, tp),
        )

    def hand_over(to):
        return remote(
            final.at[pl.ds(to * rows, rows), :], columns.at[tp], fin_send.at[0], fin_recv.at[tp], at(sp, to)
        )

    def flag(words, position):
        return lax.rem(lax.shift_right_logical(jnp.where(at_end, words[0], words[1]), position), 2)

    x_first_words = [sum(1 << (2 * height + second) for height, second in chosen) for chosen in x_first]
    near_words, far_words = comes_along_z(*x_first)

    def toward_home(code):
        tile, h = lax.div(code, 2), lax.rem(code, 2)
        relative, second = lax.div(tile, 4), lax.rem(tile, 2)
        height, group, yy = tile_at(tile)
        own_rows = own_half(yy, h)
        own_side = lax.rem(lax.div(tile, 2), 2) == 0
        over_x = (relative == 0) | (flag(x_first_words, 2 * relative + second) == 1)
        near, far = flag(near_words, tile), flag(far_words, tile)
        total[...] = part[group, own_rows, :].astype(f32)
        for count in (1, 2):

            @pl.when(near + far == count)
            def _():
                wait_chain(count, group, yy, h)

        for side, comes in enumerate((near, far)):

            @pl.when(comes == 1)
            def _():
                total[...] = total[...] + chain_in[side, group, own_rows, :].astype(f32)

        @pl.when(own_side & over_x)
        def _():
            x_copy(group, yy, h).wait_recv()
            total[...] = total[...] + x_in[height, own_rows, :].astype(f32)

        @pl.when(group != sp)
        def _():
            part[group, own_rows, :] = total[...].astype(bf16)

            @pl.when(own_side | jnp.logical_not(over_x))
            def _():
                chain_copy(group, yy, h).start()

            @pl.when(jnp.logical_not(own_side) & over_x)
            def _():
                x_copy(group, yy, h).start()

        @pl.when(group == sp)
        def _():
            final[own_rows, :] = total[...].astype(bf16)
            for to in range(4):

                @pl.when((tp != to) & (2 * yy + h == to))
                def _():
                    hand_over(to).start()

    acts = (take, take_across, pass_held, gated_units, relay_units, project_down, toward_home)

    def four_events(position, carry):
        word = pick(at_end, plans, position)

        def event(i, carry):
            code = lax.shift_right_logical(word, 8 * i) & 255
            kind, rest = lax.div(code, 32), lax.rem(code, 32)
            for j, act in enumerate(acts):

                @pl.when(kind == j)
                def _():
                    act(rest)

            return carry

        return lax.fori_loop(0, 4, event, carry)

    plans = [words_of(plan) for plan in (end_plan, middle_plan)]
    lax.fori_loop(0, max(len(plan) for plan in plans), four_events, 0)

    columns[tp] = final[pl.ds(pl.multiple_of(tp * rows, rows), rows), :]
    for by in (1, 2, 3):
        whose = lax.rem(tp + by, 4)
        remote(
            final.at[pl.ds(0, rows), :], columns.at[whose], fin_send.at[0], fin_recv.at[whose], at(sp, sibling)
        ).wait_recv()
    loaded("post_gain")
    combined = jnp.concatenate([columns[k] for k in range(4)], 1).astype(f32)
    result_ref[...] = (
        resid[...].astype(f32) + scaled_norm(combined, post_gain_ref[...].reshape(1, width))
    ).astype(bf16)

    @pl.when(sp < sp_count - 1)
    def _():
        rim_copy.wait_send()

    remote(pair_send, pair_in, pair_sem.at[0], pair_recv.at[0], at(sp, sibling)).wait_send()
    remote(y_send, y_in, y_sem.at[0], y_recv.at[0], at(sp, opposite)).wait_send()
    sent(4, 1, rows).wait_send()
    sent(3, heights, seq).wait_send()
    sent(2, heights, half).wait_send()

    def scales_sent(way, group_count):
        blocks = scales.at[pl.ds(0, group_count)]
        remote(blocks, blocks, scale_send.at[way], scale_recv.at[0], devices[way]).wait_send()

    scales_sent(2, heights)
    for count in range(1, heights):
        for way, its in enumerate((z == count - 1, z == heights - count)):

            @pl.when(its)
            def _():
                sent(way, count, half).wait_send()
                scales_sent(way, count)

    for way in range(3):
        tiles = hidden.at[:, 0]
        receive = mate_hid_recv.at[0, 0] if way else hid_recv.at[0, 0]
        remote(tiles, tiles, hid_send.at[way], receive, at(sp, sibling)).wait_send()
    for chosen, its in zip(x_first, (at_end, jnp.logical_not(at_end))):

        @pl.when(its)
        def _():
            crossed = part.at[pl.ds(0, len(chosen) + 2), pl.ds(0, half), :]
            remote(crossed, crossed, x_send.at[0], x_recv.at[0, 0, 0], at(across, tp)).wait_send()
            rising = 2 * (sp_count - 2) - len(chosen)
            across_count = 1 if rising <= sp_count else 2 if rising % 2 == 0 else 3
            chained = hidden.at[pl.ds(0, rising // across_count), pl.ds(0, across_count), pl.ds(0, half), :]
            remote(chained, chained, chain_send.at[0], chain_recv.at[0, 0, 0], at(sp, sibling)).wait_send()

    handed = final.at[pl.ds(0, 3 * rows), :]
    remote(handed, handed, fin_send.at[0], fin_recv.at[0], at(sp, sibling)).wait_send()


def dense_layer(
    stream_in,
    pre_gate,
    value_in,
    post_gate,
    conv_taps,
    out_weight,
    route_ids,
    route_weight,
    ffn_gain,
    post_gain,
    gate_proj,
    up_proj,
    down_proj,
):
    sp_count = lax.axis_size("sp")
    rows, width = stream_in.shape
    seq, channels = pre_gate.shape
    units = gate_proj.shape[2]
    cols = down_proj.shape[2]
    bf16, f32 = jnp.bfloat16, jnp.float32
    dma = pltpu.SemaphoreType.DMA
    small = (
        stream_in, pre_gate, value_in, post_gate, conv_taps, route_ids.T, route_weight.T, ffn_gain, post_gain
    )
    scratch = [pltpu.VMEM(array.shape, array.dtype) for array in small] + [
        pltpu.VMEM(out_weight.shape, bf16),
        pltpu.VMEM(gate_proj.shape[1:], bf16),
        pltpu.VMEM(up_proj.shape[1:], bf16),
        pltpu.VMEM(down_proj.shape[1:], bf16),
        pltpu.VMEM((16, channels), bf16),
        pltpu.VMEM((16, channels), bf16),
        pltpu.VMEM((seq + 8, channels), f32),
        pltpu.VMEM((seq, channels), bf16),
        pltpu.VMEM((2 * rows, width), bf16),
        pltpu.VMEM((2 * rows, width), bf16),
        pltpu.VMEM((2 * rows, width), f32),
        pltpu.VMEM((rows, width), bf16),
        pltpu.VMEM((rows, width), bf16),
        pltpu.VMEM((rows, width), bf16),
        pltpu.VMEM((sp_count, sp_count, seq), f32),
        pltpu.VMEM((sp_count, seq, width), bf16),
        pltpu.VMEM((sp_count, 4, seq, units), bf16),
        pltpu.VMEM((sp_count, seq, cols), bf16),
        pltpu.VMEM((2, sp_count, seq, cols), bf16),
        pltpu.VMEM((sp_count // 2, seq, cols), bf16),
        pltpu.VMEM((rows, cols), f32),
        pltpu.VMEM((seq, cols), bf16),
        pltpu.VMEM((4, rows, cols), bf16),
        dma((13,)),
        dma((2,)),
        dma((1,)),
        dma((4,)),
        dma((1,)),
        dma((PIECES,)),
        dma((3,)),
        dma((sp_count,)),
        dma((5,)),
        dma((sp_count, 2, PIECES)),
        dma((sp_count, 2)),
        dma((3,)),
        dma((sp_count, 2)),
        dma((sp_count, 2)),
        dma((1,)),
        dma((sp_count, 2, 2)),
        dma((1,)),
        dma((sp_count // 2, 2, 2)),
        dma((1,)),
        dma((4,)),
    ]
    vmem = pl.BlockSpec(memory_space=pltpu.VMEM)
    anywhere = pl.BlockSpec(memory_space=pl.ANY)
    return pl.pallas_call(
        functools.partial(layer_kernel, sp_count),
        out_shape=jax.ShapeDtypeStruct((rows, width), bf16),
        in_specs=[anywhere] * 13,
        out_specs=vmem,
        scratch_shapes=scratch,
        compiler_params=pltpu.CompilerParams(
            collective_id=0, has_side_effects=True, vmem_limit_bytes=58 * 1024 * 1024
        ),
    )(
        *small,
        out_weight,
        gate_proj,
        up_proj,
        down_proj,
    )


def local(
    stream_in,
    pre_gate,
    value_in,
    post_gate,
    conv_taps,
    out_weight,
    route_ids,
    route_weight,
    ffn_gain,
    post_gain,
    gate_proj,
    up_proj,
    down_proj,
):
    sp_count = lax.axis_size("sp")
    tp_count = lax.axis_size("tp")
    seq_rows = pre_gate.shape[0]
    own_rows = seq_rows // tp_count
    top_count = route_ids.shape[1]
    slots_each = 2 * own_rows * top_count // sp_count
    if tp_count == 4 and sp_count == PLANNED_GROUPS and slots_each >= own_rows:
        return dense_layer(
            stream_in, pre_gate, value_in, post_gate, conv_taps, out_weight, route_ids, route_weight,
            ffn_gain, post_gain, gate_proj, up_proj, down_proj,
        )
    tap_count = conv_taps.shape[0]
    gated_input = (pre_gate.astype(jnp.float32) * value_in.astype(jnp.float32)).astype(jnp.bfloat16)
    rim_rows = passed_along(gated_input[seq_rows - tap_count + 1 :], "sp", 1)
    padded = jnp.concatenate([rim_rows, gated_input], 0).astype(jnp.float32)
    convolved = jnp.zeros(gated_input.shape, jnp.float32)
    for tap_index in range(tap_count):
        convolved = (
            convolved
            + conv_taps[tap_index].astype(jnp.float32)[None, :]
            * padded[tap_index : tap_index + seq_rows]
        )
    mixer_out = (post_gate.astype(jnp.float32) * convolved).astype(jnp.bfloat16)
    weight_rows = mixer_out
    projected = lax.psum_scatter(
        jnp.dot(weight_rows, out_weight, preferred_element_type=jnp.float32),
        "tp",
        scatter_dimension=0,
        tiled=True,
    )
    residual = (stream_in.astype(jnp.float32) + projected).astype(jnp.bfloat16)
    normed = scaled_norm(residual.astype(jnp.float32), ffn_gain).astype(jnp.bfloat16)
    slot_rank = block_ranks(route_ids, sp_count, own_rows)
    block_of = (jnp.arange(seq_rows, dtype=jnp.int32) // own_rows)[:, None]
    tp_index = lax.axis_index("tp")
    own_ids = lax.dynamic_slice_in_dim(route_ids, tp_index * own_rows, own_rows, 0)
    own_rank = lax.dynamic_slice_in_dim(slot_rank, tp_index * own_rows, own_rows, 0)
    own_slot = own_ids * slots_each + own_rank
    picker = slot_picker(own_slot, sp_count * slots_each)
    outgoing = jnp.dot(picker, normed, preferred_element_type=jnp.float32).astype(jnp.bfloat16)
    arrived = lax.all_to_all(outgoing, "sp", split_axis=0, concat_axis=0, tiled=True)
    portion = lax.all_gather(arrived, "tp", axis=0, tiled=True)
    gate_pre = jnp.dot(portion, gate_proj[0], preferred_element_type=jnp.float32)
    up_pre = jnp.dot(portion, up_proj[0], preferred_element_type=jnp.float32)
    hidden = clamped_units(gate_pre, up_pre).astype(jnp.bfloat16)
    weight_rows = down_proj[0]
    column_out = jnp.dot(
        lax.all_gather(hidden, "tp", axis=1, tiled=True),
        weight_rows,
        preferred_element_type=jnp.float32,
    ).astype(jnp.bfloat16)
    column_width = column_out.shape[1]
    returned = lax.all_to_all(
        column_out.reshape(tp_count, sp_count, slots_each, column_width),
        "sp",
        split_axis=1,
        concat_axis=1,
        tiled=True,
    )
    home_index = (block_of * sp_count + route_ids) * slots_each + slot_rank
    gathered_out = jnp.take(returned.reshape(-1, column_width), home_index.reshape(-1), axis=0)
    gathered_out = gathered_out.astype(jnp.float32).reshape(seq_rows, top_count, column_width)
    combined_cols = jnp.sum(gathered_out * route_weight[:, :, None], axis=1).astype(jnp.bfloat16)
    combined = lax.all_to_all(combined_cols, "tp", split_axis=0, concat_axis=1, tiled=True)
    layer_out = residual.astype(jnp.float32) + scaled_norm(combined.astype(jnp.float32), post_gain)
    return layer_out.astype(jnp.bfloat16)


def solution(mesh):
    placed = (
        P(("sp", "tp"), None),
        P("sp", "tp"),
        P("sp", "tp"),
        P("sp", "tp"),
        P(None, "tp"),
        P("tp", None),
        P("sp", None),
        P("sp", None),
        P(),
        P(),
        P("sp", None, "tp"),
        P("sp", None, "tp"),
        P("sp", None, "tp"),
    )
    return jax.shard_map(
        local, mesh=mesh, in_specs=placed, out_specs=P(("sp", "tp"), None), check_vma=False
    )
```

```python
import functools

import jax
import jax.numpy as jnp
from jax import lax
from jax.experimental import pallas as pl
from jax.experimental.pallas import tpu as pltpu
from jax.sharding import PartitionSpec as P

clamp_limit = 7.0
sigmoid_scale = 1.702
epsilon = 1e-06


def passed_along(array, axis, by):
    count = lax.axis_size(axis)
    pairs = [(i, i + by) for i in range(count) if 0 <= i + by < count]
    return lax.ppermute(array, axis, pairs)


def clamped_units(gate_pre, up_pre):
    gate_cut = jnp.minimum(gate_pre, clamp_limit)
    up_cut = jnp.clip(up_pre, -clamp_limit, clamp_limit)
    return (up_cut + 1.0) * (gate_cut * jax.nn.sigmoid(sigmoid_scale * gate_cut))


def scaled_norm(values, gain):
    return (
        values
        * lax.rsqrt(jnp.mean(values * values, axis=-1, keepdims=True) + epsilon)
        * gain.astype(jnp.float32)
    )


def block_ranks(route_rows, experts, block_rows):
    flattened = route_rows.reshape(-1)
    entries = flattened.shape[0]
    span_width = block_rows * route_rows.shape[1]
    onehot = (flattened[:, None] == jnp.arange(experts, dtype=jnp.int32)[None, :]).astype(jnp.int32)
    blocked = onehot.reshape(entries // span_width, span_width, experts)
    before = jnp.cumsum(blocked, axis=1) - blocked
    return jnp.sum(before * blocked, axis=2).reshape(route_rows.shape)


def slot_picker(slot_index, table_size):
    matches = slot_index[None, :, :] == jnp.arange(table_size, dtype=jnp.int32)[:, None, None]
    return jnp.any(matches, axis=2).astype(jnp.bfloat16)


PIECES = 4
PLANNED_GROUPS = 8
end_plan = (
    8, 4, 96, 9, 10, 6, 11, 5, 100, 7, 16, 17, 97, 19, 18, 25, 133, 104, 40, 26,
    27, 102, 129, 24, 108, 28, 48, 29, 128, 135, 106, 31, 30, 13, 109, 56, 141, 110, 32, 12,
    14, 173, 60, 15, 218, 20, 139, 161, 140, 101, 172, 219, 21, 165, 203, 111, 22, 143, 23, 44,
    175, 67, 223, 103, 217, 160, 216, 66, 105, 222, 167, 52, 64, 65, 142, 107, 134, 137, 174, 221,
    171, 215, 98, 220, 166, 136, 214, 36, 204, 207, 206, 169, 99, 138, 205, 132, 168, 210, 170, 213,
    211, 164, 212, 131, 202, 163, 198, 209, 130, 199, 208, 162, 196, 200, 201, 194, 197, 195, 192, 193,
)
middle_plan = (
    8, 17, 9, 16, 96, 18, 10, 11, 19, 5, 100, 25, 12, 26, 104, 6, 13, 27, 4, 7,
    24, 14, 15, 97, 28, 29, 101, 40, 137, 31, 30, 102, 69, 68, 133, 70, 71, 108, 109, 56,
    32, 20, 48, 22, 110, 44, 141, 21, 23, 103, 66, 105, 60, 140, 111, 67, 143, 132, 64, 172,
    128, 129, 173, 134, 136, 106, 65, 175, 135, 218, 165, 52, 164, 167, 142, 223, 107, 166, 222, 174,
    139, 219, 98, 207, 171, 202, 221, 36, 215, 214, 206, 169, 205, 204, 220, 138, 99, 170, 217, 213,
    212, 131, 203, 160, 216, 210, 163, 168, 198, 211, 130, 201, 199, 161, 162, 200, 197, 209, 194, 196,
    208, 195, 193, 192,
)
x_first = (
    ((1, 0), (2, 0), (2, 1),),
    ((2, 0), (3, 0),),
)

def comes_along_z(x_first_end, x_first_middle):
    near, far = [0, 0], [0, 0]
    for tile in range(16):
        height, across, second = tile // 4, tile // 2 % 2, tile % 2
        if height == 0 and not (across and (1, second) in x_first_middle):
            far[0] |= 1 << tile
        if not (across and (height or 1, second) in x_first_end) and height != 1:
            near[1] |= 1 << tile
        if height < 2 and not (across and ((2, 3)[height], second) in x_first_middle):
            far[1] |= 1 << tile
    return near, far


def words_of(plan):
    codes = list(plan)
    codes += [255] * (-len(codes) % 4)
    words = [sum(code << (8 * i) for i, code in enumerate(codes[at : at + 4])) for at in range(0, len(codes), 4)]
    return [word - (1 << 32) if word >> 31 else word for word in words]


def pick(at_end, tables, position):
    value = jnp.int32(-1)
    for i, table in enumerate(tables):
        chosen = jnp.int32(-1)
        for j, word in enumerate(table):
            chosen = jnp.where(position == j, word, chosen)
        value = jnp.where(at_end == (i == 0), chosen, value)
    return value


def layer_kernel(
    sp_count,
    stream_hbm,
    pre_hbm,
    value_hbm,
    post_hbm,
    taps_hbm,
    ids_hbm,
    weight_hbm,
    gain_hbm,
    post_gain_hbm,
    out_hbm,
    gate_hbm,
    up_hbm,
    down_hbm,
    result_ref,
    stream_ref,
    pre_ref,
    value_ref,
    post_ref,
    taps_ref,
    ids_ref,
    weight_ref,
    gain_ref,
    post_gain_ref,
    out_w,
    gate_w,
    up_w,
    down_w,
    tail,
    rim,
    padded,
    mixed,
    pair_send,
    pair_in,
    own_sum,
    y_send,
    y_in,
    resid,
    scales,
    tokens,
    hidden,
    part,
    chain_in,
    x_in,
    total,
    final,
    columns,
    load_sem,
    rim_sem,
    pair_sem,
    pair_recv,
    y_sem,
    y_recv,
    scale_send,
    scale_recv,
    tok_send,
    tok_recv,
    across_recv,
    mate_recv,
    hid_send,
    hid_recv,
    mate_hid_recv,
    chain_send,
    chain_recv,
    x_send,
    x_recv,
    fin_send,
    fin_recv,
):
    f32, bf16 = jnp.float32, jnp.bfloat16
    heights = sp_count // 2
    last = heights - 1
    sp = lax.axis_index("sp")
    tp = lax.axis_index("tp")
    z, x = lax.div(sp, 2), lax.rem(sp, 2)
    y, c = lax.div(tp, 2), lax.rem(tp, 2)
    across, sibling = sp + 1 - 2 * x, tp + 1 - 2 * c
    opposite = lax.rem(tp + 2, 4)
    rows, width = stream_ref.shape
    seq = 4 * rows
    half = 2 * rows
    step = rows // PIECES
    units = gate_w.shape[1]
    at_end = (z == 0) | (z == last)
    toward = jnp.where(2 * z < heights, 1, -1)

    def at(sp_to, tp_to):
        return {"sp": sp_to, "tp": tp_to}

    def remote(source, target, send, receive, device):
        return pltpu.make_async_remote_copy(
            src_ref=source,
            dst_ref=target,
            send_sem=send,
            recv_sem=receive,
            device_id=device,
            device_id_type=pl.DeviceIdType.MESH,
        )

    sources = dict(
        pre=(pre_hbm, pre_ref),
        value=(value_hbm, value_ref),
        ids=(ids_hbm, ids_ref),
        weight=(weight_hbm, weight_ref),
        taps=(taps_hbm, taps_ref),
        post=(post_hbm, post_ref),
        out=(out_hbm, out_w),
        stream=(stream_hbm, stream_ref),
        gain=(gain_hbm, gain_ref),
        gate=(gate_hbm.at[0], gate_w),
        up=(up_hbm.at[0], up_w),
        down=(down_hbm.at[0], down_w),
        post_gain=(post_gain_hbm, post_gain_ref),
    )
    loads = {
        name: pltpu.make_async_copy(source, target, load_sem.at[i])
        for i, (name, (source, target)) in enumerate(sources.items())
    }
    for load in loads.values():
        load.start()

    def loaded(*wanted):
        for name in wanted:
            loads[name].wait()

    barrier = pltpu.get_barrier_semaphore()

    def greet(partner):
        pl.semaphore_signal(barrier, inc=1, device_id=partner, device_id_type=pl.DeviceIdType.MESH)

    for partner in (at(across, tp), at(sp, sibling), at(sp, opposite), at(sp, 3 - tp)):
        greet(partner)
    met = jnp.int32(4)
    for there, by in ((sp < sp_count - 1, 1), (sp > 0, -1), (z < last, 2), (z > 0, -2)):

        @pl.when(there)
        def _():
            greet(at(sp + by, tp))

        met = met + jnp.where(there, 1, 0)
    pl.semaphore_wait(barrier, met)

    loaded("pre", "value")
    gated = (pre_ref[...].astype(f32) * value_ref[...].astype(f32)).astype(bf16)
    tail[...] = gated[seq - 16 :]
    rim_copy = remote(tail, rim, rim_sem.at[0], rim_sem.at[1], at(sp + 1, tp))

    @pl.when(sp < sp_count - 1)
    def _():
        rim_copy.start()

    loaded("ids", "weight")
    expert = lax.broadcasted_iota(jnp.int32, (sp_count, seq), 0)
    spread = jnp.zeros((sp_count, seq), f32)
    for k in range(ids_ref.shape[0]):
        spread = spread + jnp.where(expert == ids_ref[k : k + 1, :], weight_ref[k : k + 1, :], 0.0)
    scales[sp] = spread

    routes = (
        lambda group: (lax.div(group, 2) <= z) & (z < last),
        lambda group: (lax.div(group, 2) >= z) & (z > 0),
    )
    devices = (at(sp + 2, tp), at(sp - 2, tp), at(across, tp), at(sp, sibling), at(sp, opposite))

    def scale_copy(way, group):
        return remote(scales.at[group], scales.at[group], scale_send.at[way], scale_recv.at[group], devices[way])

    def send_scales(group):
        for way in range(2):

            @pl.when(routes[way](group))
            def _():
                scale_copy(way, group).start()

        scale_copy(2, group).start()

    send_scales(sp)
    padded[8:, :] = gated.astype(f32)
    padded[:8, :] = jnp.zeros((8, padded.shape[1]), f32)
    loaded("taps", "post")
    tap_count = taps_ref.shape[0]
    taps = taps_ref[...].astype(f32)

    def mix(count):
        convolved = jnp.zeros((count, padded.shape[1]), f32)
        for k in range(tap_count):
            first = 8 - tap_count + 1 + k
            convolved = convolved + taps[k : k + 1, :] * padded[first : first + count, :]
        mixed[:count, :] = (post_ref[:count, :].astype(f32) * convolved).astype(bf16)

    mix(seq)
    loaded("out")

    def rows_of(core):
        return jnp.concatenate(
            [mixed[pl.ds(pl.multiple_of(yy * half + core * rows, rows), rows), :] for yy in range(2)], 0
        )

    def offset_of(p):
        return lax.rem(p + 1, PIECES) * step

    def pair_copy(i):
        if i < 2:
            whose = pl.ds(pl.multiple_of(((1 - y) if i == 0 else y) * rows + step, step), rows - step)
        else:
            whose = pl.ds((3 - i) * rows, step)
        return remote(
            pair_send.at[whose, :], pair_in.at[whose, :], pair_sem.at[0], pair_recv.at[i], at(sp, sibling)
        )

    pair_send[...] = jnp.dot(rows_of(1 - c), out_w[...], preferred_element_type=f32).astype(bf16)
    for i in range(3):
        pair_copy(i).start()

    @pl.when(c == 0)
    def _():
        pair_copy(3).start()

    own_sum[...] = jnp.dot(rows_of(c), out_w[...], preferred_element_type=f32)

    def pair_sum(yy, p):
        piece = pl.ds(pl.multiple_of(yy * rows + offset_of(p), step), step)
        return own_sum[piece, :] + pair_in[piece, :].astype(f32)

    def y_copy(p):
        piece = pl.ds(pl.multiple_of(offset_of(p), step), step)
        return remote(y_send.at[piece, :], y_in.at[piece, :], y_sem.at[0], y_recv.at[p], at(sp, opposite))

    def send_y(p):
        y_send[pl.ds(pl.multiple_of(offset_of(p), step), step), :] = pair_sum(1 - y, p).astype(bf16)
        y_copy(p).start()

    pair_copy(0).wait_recv()
    for p in range(PIECES - 1):
        send_y(p)

    @pl.when(sp > 0)
    def _():
        rim_copy.wait_recv()
        padded[:8, :] = rim[...].astype(f32)[8:]

    mix(step)
    first_rows = jnp.dot(mixed[:step, :], out_w[...], preferred_element_type=f32)

    @pl.when(c == 0)
    def _():
        own_sum[:step, :] = first_rows

    @pl.when(c == 1)
    def _():
        pair_send[:step, :] = first_rows.astype(bf16)
        pair_copy(3).start()

    for i in (2, 3):
        pair_copy(i).wait_recv()
    send_y(PIECES - 1)
    pair_copy(1).wait_recv()
    loaded("stream", "gain")

    def height_of(relative):
        inner = jnp.where(relative == 0, 0, jnp.where(relative == 1, -1, relative - 1))
        return z + toward * jnp.where(at_end, relative, inner)

    def wait_scales(group):
        scale_copy(2, group).wait_recv()

    def piece_of(group, yy, p):
        return tokens.at[group, pl.ds(pl.multiple_of((2 * yy + c) * rows + offset_of(p), step), step), :]

    def block_of(group, yy, core):
        return tokens.at[group, pl.ds(pl.multiple_of((2 * yy + core) * rows, rows), rows), :]

    def pass_on(way, group, yy, p):
        piece = piece_of(group, yy, p)
        height = lax.div(group, 2)
        if way == 2:
            receive = across_recv.at[height, yy]
        elif way == 3:
            receive = mate_recv.at[group, yy]
        else:
            receive = tok_recv.at[height, yy, p]
        return remote(piece, piece, tok_send.at[way], receive, devices[way])

    def sent(way, group_count, row_count):
        rows_sent = tokens.at[pl.ds(0, group_count), pl.ds(0, row_count), :]
        return remote(rows_sent, rows_sent, tok_send.at[way], mate_recv.at[0, 0], devices[way])

    def along_z(group, yy, p):
        for way in range(2):

            @pl.when(routes[way](group))
            def _():
                pass_on(way, group, yy, p).start()

    for p in range(PIECES):
        y_copy(p).wait_recv()
        piece = pl.ds(pl.multiple_of(offset_of(p), step), step)
        residual = (
            stream_ref[piece, :].astype(f32) + (pair_sum(y, p) + y_in[piece, :].astype(f32))
        ).astype(bf16)
        resid[piece, :] = residual
        tokens[sp, pl.ds(pl.multiple_of(tp * rows + offset_of(p), step), step), :] = scaled_norm(
            residual.astype(f32), gain_ref[...].reshape(1, width)
        ).astype(bf16)
        pass_on(4, sp, y, p).start()
        along_z(sp, y, p)
        pass_on(2, sp, y, p).start()
        pass_on(3, sp, y, p).start()

    loaded("gate", "up", "down")

    def wait_piece(group, yy, p):
        pass_on(0, group, yy, p).wait_recv()

    def wait_mate(group, yy):
        block = block_of(group, yy, 1 - c)
        remote(block, block, tok_send.at[3], mate_recv.at[group, yy], at(sp, sibling)).wait_recv()

    def block_at(code):
        relative, second, p = lax.div(code, 2 * PIECES), lax.rem(lax.div(code, PIECES), 2), lax.rem(code, PIECES)
        return relative, height_of(relative), jnp.where(second == 0, y, 1 - y), p

    def take(code):
        relative, height, yy, p = block_at(code)
        group = 2 * height + x

        @pl.when((relative > 0) & (lax.rem(code, 2 * PIECES) == 0))
        def _():
            wait_scales(group)
            send_scales(group)

        wait_piece(group, yy, p)

        @pl.when((relative > 0) | at_end)
        def _():
            along_z(group, yy, p)

        pass_on(3, group, yy, p).start()

        @pl.when(relative > 0)
        def _():
            pass_on(2, group, yy, p).start()

    def take_across(code):
        _, height, yy, _ = block_at(code)
        group = 2 * height + 1 - x

        @pl.when(lax.rem(code, 2 * PIECES) == 0)
        def _():
            wait_scales(group)

        block = block_of(group, yy, c)
        remote(block, block, tok_send.at[2], across_recv.at[height, yy], devices[2]).wait_recv()
        remote(block, block, tok_send.at[3], mate_recv.at[group, yy], devices[3]).start()

    def pass_held(code):
        p = lax.rem(code, PIECES)

        @pl.when(code < PIECES)
        def _():
            pass_on(2, sp, 1 - y, p).start()

        @pl.when(code >= PIECES)
        def _():
            along_z(sp, 1 - y, p)

    def tile_at(tile):
        height = height_of(lax.div(tile, 4))
        side = jnp.where(lax.rem(lax.div(tile, 2), 2) == 0, x, 1 - x)
        return height, 2 * height + side, jnp.where(lax.rem(tile, 2) == 0, y, 1 - y)

    def tile_rows(yy):
        return pl.ds(pl.multiple_of(yy * half, half), half)

    def share(way, group, yy):
        whose = tp if way < 2 else opposite
        block = hidden.at[group, whose, tile_rows(yy), :]
        receive = mate_hid_recv.at[group, yy] if way else hid_recv.at[group, yy]
        return remote(block, block, hid_send.at[way], receive, at(sp, sibling if way else opposite))

    def gated_units(tile):
        _, group, yy = tile_at(tile)
        wait_mate(group, yy)
        inputs = tokens[group, tile_rows(yy), :]
        span = min(256, units)
        for start in range(0, units, span):
            gate_pre = jnp.dot(inputs, gate_w[:, start : start + span], preferred_element_type=f32)
            up_pre = jnp.dot(inputs, up_w[:, start : start + span], preferred_element_type=f32)
            hidden[group, tp, tile_rows(yy), start : start + span] = clamped_units(gate_pre, up_pre).astype(bf16)
        share(0, group, yy).start()
        share(1, group, yy).start()

    def relay_units(tile):
        _, group, yy = tile_at(tile)
        share(0, group, yy).wait_recv()
        share(2, group, yy).start()

    def own_half(yy, h):
        return pl.ds(pl.multiple_of(yy * half + h * rows, rows), rows)

    def chain_copy(group, yy, h):
        rising = lax.div(group, 2) > z
        return remote(
            part.at[group, own_half(yy, h), :],
            chain_in.at[jnp.where(at_end, 0, 1), group, own_half(yy, h), :],
            chain_send.at[0],
            chain_recv.at[group, yy, h],
            at(sp + jnp.where(rising, 2, -2), tp),
        )

    def wait_chain(sides, group, yy, h):
        tiles = chain_in.at[pl.ds(0, sides), group, own_half(yy, h), :]
        remote(tiles, tiles, chain_send.at[0], chain_recv.at[group, yy, h], at(sp, sibling)).wait_recv()

    diagonal = lax.broadcasted_iota(jnp.int32, (half, half), 0) == lax.broadcasted_iota(jnp.int32, (half, half), 1)

    def project_down(tile):
        _, group, yy = tile_at(tile)
        both = hidden.at[group, pl.ds(0, 2), tile_rows(yy), :]
        remote(both, both, hid_send.at[1], mate_hid_recv.at[group, yy], at(sp, sibling)).wait_recv()
        own_rows = tile_rows(yy)
        out = jnp.dot(hidden[group, 0, own_rows, :], down_w[:units, :], preferred_element_type=f32)
        for k in range(1, 4):
            out = out + jnp.dot(
                hidden[group, k, own_rows, :], down_w[k * units : (k + 1) * units, :], preferred_element_type=f32
            )
        weight = scales[group, :, tile_rows(yy)]
        mine = lax.broadcasted_iota(jnp.int32, weight.shape, 0) == sp
        weight = jnp.sum(jnp.where(mine, weight, 0.0), axis=0, keepdims=True)
        weight = jnp.sum(jnp.where(diagonal, weight, 0.0), axis=1, keepdims=True)
        part[group, own_rows, :] = (out.astype(bf16).astype(f32) * weight).astype(bf16)

    def x_copy(group, yy, h):
        height = lax.div(group, 2)
        return remote(
            part.at[group, own_half(yy, h), :],
            x_in.at[height, own_half(yy, h), :],
            x_send.at[0],
            x_recv.at[height, yy, h],
            at(across, tp),
        )

    def hand_over(to):
        return remote(
            final.at[pl.ds(to * rows, rows), :], columns.at[tp], fin_send.at[0], fin_recv.at[tp], at(sp, to)
        )

    def flag(words, position):
        return lax.rem(lax.shift_right_logical(jnp.where(at_end, words[0], words[1]), position), 2)

    x_first_words = [sum(1 << (2 * height + second) for height, second in chosen) for chosen in x_first]
    near_words, far_words = comes_along_z(*x_first)

    def toward_home(code):
        tile, h = lax.div(code, 2), lax.rem(code, 2)
        relative, second = lax.div(tile, 4), lax.rem(tile, 2)
        height, group, yy = tile_at(tile)
        own_rows = own_half(yy, h)
        own_side = lax.rem(lax.div(tile, 2), 2) == 0
        over_x = (relative == 0) | (flag(x_first_words, 2 * relative + second) == 1)
        near, far = flag(near_words, tile), flag(far_words, tile)
        total[...] = part[group, own_rows, :].astype(f32)
        for count in (1, 2):

            @pl.when(near + far == count)
            def _():
                wait_chain(count, group, yy, h)

        for side, comes in enumerate((near, far)):

            @pl.when(comes == 1)
            def _():
                total[...] = total[...] + chain_in[side, group, own_rows, :].astype(f32)

        @pl.when(own_side & over_x)
        def _():
            x_copy(group, yy, h).wait_recv()
            total[...] = total[...] + x_in[height, own_rows, :].astype(f32)

        @pl.when(group != sp)
        def _():
            part[group, own_rows, :] = total[...].astype(bf16)

            @pl.when(own_side | jnp.logical_not(over_x))
            def _():
                chain_copy(group, yy, h).start()

            @pl.when(jnp.logical_not(own_side) & over_x)
            def _():
                x_copy(group, yy, h).start()

        @pl.when(group == sp)
        def _():
            final[own_rows, :] = total[...].astype(bf16)
            for to in range(4):

                @pl.when((tp != to) & (2 * yy + h == to))
                def _():
                    hand_over(to).start()

    acts = (take, take_across, pass_held, gated_units, relay_units, project_down, toward_home)

    def four_events(position, carry):
        word = pick(at_end, plans, position)

        def event(i, carry):
            code = lax.shift_right_logical(word, 8 * i) & 255
            kind, rest = lax.div(code, 32), lax.rem(code, 32)
            for j, act in enumerate(acts):

                @pl.when(kind == j)
                def _():
                    act(rest)

            return carry

        return lax.fori_loop(0, 4, event, carry)

    plans = [words_of(plan) for plan in (end_plan, middle_plan)]
    lax.fori_loop(0, max(len(plan) for plan in plans), four_events, 0)

    columns[tp] = final[pl.ds(pl.multiple_of(tp * rows, rows), rows), :]
    for by in (1, 2, 3):
        whose = lax.rem(tp + by, 4)
        remote(
            final.at[pl.ds(0, rows), :], columns.at[whose], fin_send.at[0], fin_recv.at[whose], at(sp, sibling)
        ).wait_recv()
    loaded("post_gain")
    combined = jnp.concatenate([columns[k] for k in range(4)], 1).astype(f32)
    result_ref[...] = (
        resid[...].astype(f32) + scaled_norm(combined, post_gain_ref[...].reshape(1, width))
    ).astype(bf16)

    @pl.when(sp < sp_count - 1)
    def _():
        rim_copy.wait_send()

    remote(pair_send, pair_in, pair_sem.at[0], pair_recv.at[0], at(sp, sibling)).wait_send()
    remote(y_send, y_in, y_sem.at[0], y_recv.at[0], at(sp, opposite)).wait_send()
    sent(4, 1, rows).wait_send()
    sent(3, heights, seq).wait_send()
    sent(2, heights, half).wait_send()

    def scales_sent(way, group_count):
        blocks = scales.at[pl.ds(0, group_count)]
        remote(blocks, blocks, scale_send.at[way], scale_recv.at[0], devices[way]).wait_send()

    scales_sent(2, heights)
    for count in range(1, heights):
        for way, its in enumerate((z == count - 1, z == heights - count)):

            @pl.when(its)
            def _():
                sent(way, count, half).wait_send()
                scales_sent(way, count)

    for way in range(3):
        tiles = hidden.at[:, 0]
        receive = mate_hid_recv.at[0, 0] if way else hid_recv.at[0, 0]
        remote(tiles, tiles, hid_send.at[way], receive, at(sp, sibling)).wait_send()
    for chosen, its in zip(x_first, (at_end, jnp.logical_not(at_end))):

        @pl.when(its)
        def _():
            crossed = part.at[pl.ds(0, len(chosen) + 2), pl.ds(0, half), :]
            remote(crossed, crossed, x_send.at[0], x_recv.at[0, 0, 0], at(across, tp)).wait_send()
            rising = 2 * (sp_count - 2) - len(chosen)
            across_count = 1 if rising <= sp_count else 2 if rising % 2 == 0 else 3
            chained = hidden.at[pl.ds(0, rising // across_count), pl.ds(0, across_count), pl.ds(0, half), :]
            remote(chained, chained, chain_send.at[0], chain_recv.at[0, 0, 0], at(sp, sibling)).wait_send()

    handed = final.at[pl.ds(0, 3 * rows), :]
    remote(handed, handed, fin_send.at[0], fin_recv.at[0], at(sp, sibling)).wait_send()


def dense_layer(
    stream_in,
    pre_gate,
    value_in,
    post_gate,
    conv_taps,
    out_weight,
    route_ids,
    route_weight,
    ffn_gain,
    post_gain,
    gate_proj,
    up_proj,
    down_proj,
):
    sp_count = lax.axis_size("sp")
    rows, width = stream_in.shape
    seq, channels = pre_gate.shape
    units = gate_proj.shape[2]
    cols = down_proj.shape[2]
    bf16, f32 = jnp.bfloat16, jnp.float32
    dma = pltpu.SemaphoreType.DMA
    small = (
        stream_in, pre_gate, value_in, post_gate, conv_taps, route_ids.T, route_weight.T, ffn_gain, post_gain
    )
    scratch = [pltpu.VMEM(array.shape, array.dtype) for array in small] + [
        pltpu.VMEM(out_weight.shape, bf16),
        pltpu.VMEM(gate_proj.shape[1:], bf16),
        pltpu.VMEM(up_proj.shape[1:], bf16),
        pltpu.VMEM(down_proj.shape[1:], bf16),
        pltpu.VMEM((16, channels), bf16),
        pltpu.VMEM((16, channels), bf16),
        pltpu.VMEM((seq + 8, channels), f32),
        pltpu.VMEM((seq, channels), bf16),
        pltpu.VMEM((2 * rows, width), bf16),
        pltpu.VMEM((2 * rows, width), bf16),
        pltpu.VMEM((2 * rows, width), f32),
        pltpu.VMEM((rows, width), bf16),
        pltpu.VMEM((rows, width), bf16),
        pltpu.VMEM((rows, width), bf16),
        pltpu.VMEM((sp_count, sp_count, seq), f32),
        pltpu.VMEM((sp_count, seq, width), bf16),
        pltpu.VMEM((sp_count, 4, seq, units), bf16),
        pltpu.VMEM((sp_count, seq, cols), bf16),
        pltpu.VMEM((2, sp_count, seq, cols), bf16),
        pltpu.VMEM((sp_count // 2, seq, cols), bf16),
        pltpu.VMEM((rows, cols), f32),
        pltpu.VMEM((seq, cols), bf16),
        pltpu.VMEM((4, rows, cols), bf16),
        dma((13,)),
        dma((2,)),
        dma((1,)),
        dma((4,)),
        dma((1,)),
        dma((PIECES,)),
        dma((3,)),
        dma((sp_count,)),
        dma((5,)),
        dma((sp_count // 2, 2, PIECES)),
        dma((sp_count // 2, 2)),
        dma((sp_count, 2)),
        dma((3,)),
        dma((sp_count, 2)),
        dma((sp_count, 2)),
        dma((1,)),
        dma((sp_count, 2, 2)),
        dma((1,)),
        dma((sp_count // 2, 2, 2)),
        dma((1,)),
        dma((4,)),
    ]
    vmem = pl.BlockSpec(memory_space=pltpu.VMEM)
    anywhere = pl.BlockSpec(memory_space=pl.ANY)
    return pl.pallas_call(
        functools.partial(layer_kernel, sp_count),
        out_shape=jax.ShapeDtypeStruct((rows, width), bf16),
        in_specs=[anywhere] * 13,
        out_specs=vmem,
        scratch_shapes=scratch,
        compiler_params=pltpu.CompilerParams(
            collective_id=0, has_side_effects=True, vmem_limit_bytes=58 * 1024 * 1024
        ),
    )(
        *small,
        out_weight,
        gate_proj,
        up_proj,
        down_proj,
    )


def local(
    stream_in,
    pre_gate,
    value_in,
    post_gate,
    conv_taps,
    out_weight,
    route_ids,
    route_weight,
    ffn_gain,
    post_gain,
    gate_proj,
    up_proj,
    down_proj,
):
    sp_count = lax.axis_size("sp")
    tp_count = lax.axis_size("tp")
    seq_rows = pre_gate.shape[0]
    own_rows = seq_rows // tp_count
    top_count = route_ids.shape[1]
    slots_each = 2 * own_rows * top_count // sp_count
    if tp_count == 4 and sp_count == PLANNED_GROUPS and slots_each >= own_rows:
        return dense_layer(
            stream_in, pre_gate, value_in, post_gate, conv_taps, out_weight, route_ids, route_weight,
            ffn_gain, post_gain, gate_proj, up_proj, down_proj,
        )
    tap_count = conv_taps.shape[0]
    gated_input = (pre_gate.astype(jnp.float32) * value_in.astype(jnp.float32)).astype(jnp.bfloat16)
    rim_rows = passed_along(gated_input[seq_rows - tap_count + 1 :], "sp", 1)
    padded = jnp.concatenate([rim_rows, gated_input], 0).astype(jnp.float32)
    convolved = jnp.zeros(gated_input.shape, jnp.float32)
    for tap_index in range(tap_count):
        convolved = (
            convolved
            + conv_taps[tap_index].astype(jnp.float32)[None, :]
            * padded[tap_index : tap_index + seq_rows]
        )
    mixer_out = (post_gate.astype(jnp.float32) * convolved).astype(jnp.bfloat16)
    weight_rows = mixer_out
    projected = lax.psum_scatter(
        jnp.dot(weight_rows, out_weight, preferred_element_type=jnp.float32),
        "tp",
        scatter_dimension=0,
        tiled=True,
    )
    residual = (stream_in.astype(jnp.float32) + projected).astype(jnp.bfloat16)
    normed = scaled_norm(residual.astype(jnp.float32), ffn_gain).astype(jnp.bfloat16)
    slot_rank = block_ranks(route_ids, sp_count, own_rows)
    block_of = (jnp.arange(seq_rows, dtype=jnp.int32) // own_rows)[:, None]
    tp_index = lax.axis_index("tp")
    own_ids = lax.dynamic_slice_in_dim(route_ids, tp_index * own_rows, own_rows, 0)
    own_rank = lax.dynamic_slice_in_dim(slot_rank, tp_index * own_rows, own_rows, 0)
    own_slot = own_ids * slots_each + own_rank
    picker = slot_picker(own_slot, sp_count * slots_each)
    outgoing = jnp.dot(picker, normed, preferred_element_type=jnp.float32).astype(jnp.bfloat16)
    arrived = lax.all_to_all(outgoing, "sp", split_axis=0, concat_axis=0, tiled=True)
    portion = lax.all_gather(arrived, "tp", axis=0, tiled=True)
    gate_pre = jnp.dot(portion, gate_proj[0], preferred_element_type=jnp.float32)
    up_pre = jnp.dot(portion, up_proj[0], preferred_element_type=jnp.float32)
    hidden = clamped_units(gate_pre, up_pre).astype(jnp.bfloat16)
    weight_rows = down_proj[0]
    column_out = jnp.dot(
        lax.all_gather(hidden, "tp", axis=1, tiled=True),
        weight_rows,
        preferred_element_type=jnp.float32,
    ).astype(jnp.bfloat16)
    column_width = column_out.shape[1]
    returned = lax.all_to_all(
        column_out.reshape(tp_count, sp_count, slots_each, column_width),
        "sp",
        split_axis=1,
        concat_axis=1,
        tiled=True,
    )
    home_index = (block_of * sp_count + route_ids) * slots_each + slot_rank
    gathered_out = jnp.take(returned.reshape(-1, column_width), home_index.reshape(-1), axis=0)
    gathered_out = gathered_out.astype(jnp.float32).reshape(seq_rows, top_count, column_width)
    combined_cols = jnp.sum(gathered_out * route_weight[:, :, None], axis=1).astype(jnp.bfloat16)
    combined = lax.all_to_all(combined_cols, "tp", split_axis=0, concat_axis=1, tiled=True)
    layer_out = residual.astype(jnp.float32) + scaled_norm(combined.astype(jnp.float32), post_gain)
    return layer_out.astype(jnp.bfloat16)


def solution(mesh):
    placed = (
        P(("sp", "tp"), None),
        P("sp", "tp"),
        P("sp", "tp"),
        P("sp", "tp"),
        P(None, "tp"),
        P("tp", None),
        P("sp", None),
        P("sp", None),
        P(),
        P(),
        P("sp", None, "tp"),
        P("sp", None, "tp"),
        P("sp", None, "tp"),
    )
    return jax.shard_map(
        local, mesh=mesh, in_specs=placed, out_specs=P(("sp", "tp"), None), check_vma=False
    )
```

```python
import functools

import jax
import jax.numpy as jnp
from jax import lax
from jax.experimental import pallas as pl
from jax.experimental.pallas import tpu as pltpu
from jax.sharding import PartitionSpec as P

clamp_limit = 7.0
sigmoid_scale = 1.702
epsilon = 1e-06


def passed_along(array, axis, by):
    count = lax.axis_size(axis)
    pairs = [(i, i + by) for i in range(count) if 0 <= i + by < count]
    return lax.ppermute(array, axis, pairs)


def clamped_units(gate_pre, up_pre):
    gate_cut = jnp.minimum(gate_pre, clamp_limit)
    up_cut = jnp.clip(up_pre, -clamp_limit, clamp_limit)
    return (up_cut + 1.0) * (gate_cut * jax.nn.sigmoid(sigmoid_scale * gate_cut))


def scaled_norm(values, gain):
    return (
        values
        * lax.rsqrt(jnp.mean(values * values, axis=-1, keepdims=True) + epsilon)
        * gain.astype(jnp.float32)
    )


def block_ranks(route_rows, experts, block_rows):
    flattened = route_rows.reshape(-1)
    entries = flattened.shape[0]
    span_width = block_rows * route_rows.shape[1]
    onehot = (flattened[:, None] == jnp.arange(experts, dtype=jnp.int32)[None, :]).astype(jnp.int32)
    blocked = onehot.reshape(entries // span_width, span_width, experts)
    before = jnp.cumsum(blocked, axis=1) - blocked
    return jnp.sum(before * blocked, axis=2).reshape(route_rows.shape)


def slot_picker(slot_index, table_size):
    matches = slot_index[None, :, :] == jnp.arange(table_size, dtype=jnp.int32)[:, None, None]
    return jnp.any(matches, axis=2).astype(jnp.bfloat16)


PIECES = 4
PLANNED_GROUPS = 8
end_plan = (
    4, 8, 10, 96, 9, 11, 5, 100, 6, 7, 17, 18, 97, 40, 19, 25, 102, 16, 24, 27,
    104, 128, 26, 48, 108, 28, 129, 29, 106, 161, 56, 31, 30, 133, 109, 141, 13, 110, 173, 137,
    14, 219, 218, 32, 15, 12, 135, 60, 101, 140, 20, 165, 172, 202, 22, 111, 143, 216, 217, 23,
    21, 66, 44, 64, 67, 65, 175, 223, 222, 103, 203, 105, 142, 167, 207, 52, 174, 221, 139, 107,
    220, 134, 169, 171, 214, 98, 160, 206, 136, 36, 215, 166, 168, 205, 138, 210, 99, 170, 213, 211,
    131, 212, 132, 204, 163, 198, 209, 130, 199, 208, 162, 196, 164, 197, 201, 200, 194, 195, 192, 193,
)
middle_plan = (
    9, 8, 17, 96, 4, 18, 19, 6, 11, 10, 16, 25, 100, 7, 24, 5, 32, 13, 12, 104,
    27, 15, 14, 26, 108, 28, 29, 31, 101, 30, 71, 69, 70, 40, 68, 102, 109, 97, 20, 48,
    22, 21, 44, 23, 56, 103, 141, 140, 110, 129, 133, 132, 64, 65, 66, 173, 105, 135, 128, 67,
    219, 172, 60, 134, 111, 106, 164, 218, 143, 166, 204, 137, 165, 175, 203, 52, 205, 136, 222, 223,
    167, 107, 142, 98, 206, 139, 174, 221, 161, 36, 207, 171, 214, 215, 220, 138, 99, 169, 170, 217,
    213, 160, 212, 131, 168, 216, 202, 163, 198, 210, 211, 130, 201, 199, 162, 197, 200, 209, 196, 194,
    208, 195, 193, 192,
)
x_first = (
    ((2, 0), (2, 1),),
    ((1, 0), (2, 0), (3, 0),),
)

def comes_along_z(x_first_end, x_first_middle):
    near, far = [0, 0], [0, 0]
    for tile in range(16):
        height, across, second = tile // 4, tile // 2 % 2, tile % 2
        if height == 0 and not (across and (1, second) in x_first_middle):
            far[0] |= 1 << tile
        if not (across and (height or 1, second) in x_first_end) and height != 1:
            near[1] |= 1 << tile
        if height < 2 and not (across and ((2, 3)[height], second) in x_first_middle):
            far[1] |= 1 << tile
    return near, far


def words_of(plan):
    codes = list(plan)
    codes += [255] * (-len(codes) % 4)
    words = [sum(code << (8 * i) for i, code in enumerate(codes[at : at + 4])) for at in range(0, len(codes), 4)]
    return [word - (1 << 32) if word >> 31 else word for word in words]


def pick(at_end, tables, position):
    value = jnp.int32(-1)
    for i, table in enumerate(tables):
        chosen = jnp.int32(-1)
        for j, word in enumerate(table):
            chosen = jnp.where(position == j, word, chosen)
        value = jnp.where(at_end == (i == 0), chosen, value)
    return value


def layer_kernel(
    sp_count,
    stream_hbm,
    pre_hbm,
    value_hbm,
    post_hbm,
    taps_hbm,
    ids_hbm,
    weight_hbm,
    gain_hbm,
    post_gain_hbm,
    out_hbm,
    gate_hbm,
    up_hbm,
    down_hbm,
    result_ref,
    stream_ref,
    pre_ref,
    value_ref,
    post_ref,
    taps_ref,
    ids_ref,
    weight_ref,
    gain_ref,
    post_gain_ref,
    out_w,
    gate_w,
    up_w,
    down_w,
    tail,
    rim,
    padded,
    mixed,
    pair_send,
    pair_in,
    own_sum,
    y_send,
    y_in,
    resid,
    scales,
    tokens,
    hidden,
    part,
    chain_in,
    x_in,
    total,
    final,
    columns,
    load_sem,
    rim_sem,
    pair_sem,
    pair_recv,
    y_sem,
    y_recv,
    scale_send,
    scale_recv,
    tok_send,
    tok_recv,
    across_recv,
    mate_recv,
    hid_send,
    hid_recv,
    mate_hid_recv,
    chain_send,
    chain_recv,
    x_send,
    x_recv,
    fin_send,
    fin_recv,
):
    f32, bf16 = jnp.float32, jnp.bfloat16
    heights = sp_count // 2
    last = heights - 1
    sp = lax.axis_index("sp")
    tp = lax.axis_index("tp")
    z, x = lax.div(sp, 2), lax.rem(sp, 2)
    y, c = lax.div(tp, 2), lax.rem(tp, 2)
    across, sibling = sp + 1 - 2 * x, tp + 1 - 2 * c
    opposite = lax.rem(tp + 2, 4)
    rows, width = stream_ref.shape
    seq = 4 * rows
    half = 2 * rows
    step = rows // PIECES
    units = gate_w.shape[1]
    at_end = (z == 0) | (z == last)
    toward = jnp.where(2 * z < heights, 1, -1)

    def at(sp_to, tp_to):
        return {"sp": sp_to, "tp": tp_to}

    def remote(source, target, send, receive, device):
        return pltpu.make_async_remote_copy(
            src_ref=source,
            dst_ref=target,
            send_sem=send,
            recv_sem=receive,
            device_id=device,
            device_id_type=pl.DeviceIdType.MESH,
        )

    sources = dict(
        pre=(pre_hbm, pre_ref),
        value=(value_hbm, value_ref),
        ids=(ids_hbm, ids_ref),
        weight=(weight_hbm, weight_ref),
        taps=(taps_hbm, taps_ref),
        post=(post_hbm, post_ref),
        out=(out_hbm, out_w),
        stream=(stream_hbm, stream_ref),
        gain=(gain_hbm, gain_ref),
        gate=(gate_hbm.at[0], gate_w),
        up=(up_hbm.at[0], up_w),
        down=(down_hbm.at[0], down_w),
        post_gain=(post_gain_hbm, post_gain_ref),
    )
    loads = {
        name: pltpu.make_async_copy(source, target, load_sem.at[i])
        for i, (name, (source, target)) in enumerate(sources.items())
    }
    for load in loads.values():
        load.start()

    def loaded(*wanted):
        for name in wanted:
            loads[name].wait()

    barrier = pltpu.get_barrier_semaphore()

    def greet(partner):
        pl.semaphore_signal(barrier, inc=1, device_id=partner, device_id_type=pl.DeviceIdType.MESH)

    for partner in (at(across, tp), at(sp, sibling), at(sp, opposite), at(sp, 3 - tp)):
        greet(partner)
    met = jnp.int32(4)
    for there, by in ((sp < sp_count - 1, 1), (sp > 0, -1), (z < last, 2), (z > 0, -2)):

        @pl.when(there)
        def _():
            greet(at(sp + by, tp))

        met = met + jnp.where(there, 1, 0)
    pl.semaphore_wait(barrier, met)

    loaded("pre", "value")
    gated = (pre_ref[...].astype(f32) * value_ref[...].astype(f32)).astype(bf16)
    tail[...] = gated[seq - 16 :]
    rim_copy = remote(tail, rim, rim_sem.at[0], rim_sem.at[1], at(sp + 1, tp))

    @pl.when(sp < sp_count - 1)
    def _():
        rim_copy.start()

    routes = (
        lambda group: (lax.div(group, 2) <= z) & (z < last),
        lambda group: (lax.div(group, 2) >= z) & (z > 0),
    )
    devices = (at(sp + 2, tp), at(sp - 2, tp), at(across, tp), at(sp, sibling), at(sp, opposite))

    def scale_copy(way, group):
        return remote(scales.at[group], scales.at[group], scale_send.at[way], scale_recv.at[group], devices[way])

    def send_scales(group):
        for way in range(2):

            @pl.when(routes[way](group))
            def _():
                scale_copy(way, group).start()

        scale_copy(2, group).start()

    padded[8:, :] = gated.astype(f32)
    padded[:8, :] = jnp.zeros((8, padded.shape[1]), f32)
    loaded("taps", "post")
    tap_count = taps_ref.shape[0]
    taps = taps_ref[...].astype(f32)

    def mix(count):
        convolved = jnp.zeros((count, padded.shape[1]), f32)
        for k in range(tap_count):
            first = 8 - tap_count + 1 + k
            convolved = convolved + taps[k : k + 1, :] * padded[first : first + count, :]
        mixed[:count, :] = (post_ref[:count, :].astype(f32) * convolved).astype(bf16)

    mix(seq)
    loaded("out")

    def rows_of(core):
        return jnp.concatenate(
            [mixed[pl.ds(pl.multiple_of(yy * half + core * rows, rows), rows), :] for yy in range(2)], 0
        )

    def offset_of(p):
        return lax.rem(p + 1, PIECES) * step

    def pair_copy(i):
        if i < 2:
            whose = pl.ds(pl.multiple_of(((1 - y) if i == 0 else y) * rows + step, step), rows - step)
        else:
            whose = pl.ds((3 - i) * rows, step)
        return remote(
            pair_send.at[whose, :], pair_in.at[whose, :], pair_sem.at[0], pair_recv.at[i], at(sp, sibling)
        )

    pair_send[...] = jnp.dot(rows_of(1 - c), out_w[...], preferred_element_type=f32).astype(bf16)
    for i in range(3):
        pair_copy(i).start()

    @pl.when(c == 0)
    def _():
        pair_copy(3).start()

    own_sum[...] = jnp.dot(rows_of(c), out_w[...], preferred_element_type=f32)

    def pair_sum(yy, p):
        piece = pl.ds(pl.multiple_of(yy * rows + offset_of(p), step), step)
        return own_sum[piece, :] + pair_in[piece, :].astype(f32)

    def y_copy(p):
        piece = pl.ds(pl.multiple_of(offset_of(p), step), step)
        return remote(y_send.at[piece, :], y_in.at[piece, :], y_sem.at[0], y_recv.at[p], at(sp, opposite))

    def send_y(p):
        y_send[pl.ds(pl.multiple_of(offset_of(p), step), step), :] = pair_sum(1 - y, p).astype(bf16)
        y_copy(p).start()

    pair_copy(0).wait_recv()
    for p in range(PIECES - 1):
        send_y(p)

    loaded("ids", "weight")
    expert = lax.broadcasted_iota(jnp.int32, (sp_count, seq), 0)
    spread = jnp.zeros((sp_count, seq), f32)
    for k in range(ids_ref.shape[0]):
        spread = spread + jnp.where(expert == ids_ref[k : k + 1, :], weight_ref[k : k + 1, :], 0.0)
    scales[sp] = spread

    send_scales(sp)

    @pl.when(sp > 0)
    def _():
        rim_copy.wait_recv()
        padded[:8, :] = rim[...].astype(f32)[8:]

    mix(step)
    first_rows = jnp.dot(mixed[:step, :], out_w[...], preferred_element_type=f32)

    @pl.when(c == 0)
    def _():
        own_sum[:step, :] = first_rows

    @pl.when(c == 1)
    def _():
        pair_send[:step, :] = first_rows.astype(bf16)
        pair_copy(3).start()

    for i in (2, 3):
        pair_copy(i).wait_recv()
    send_y(PIECES - 1)
    pair_copy(1).wait_recv()
    loaded("stream", "gain")

    def height_of(relative):
        inner = jnp.where(relative == 0, 0, jnp.where(relative == 1, -1, relative - 1))
        return z + toward * jnp.where(at_end, relative, inner)

    def wait_scales(group):
        scale_copy(2, group).wait_recv()

    def piece_of(group, yy, p):
        return tokens.at[group, pl.ds(pl.multiple_of((2 * yy + c) * rows + offset_of(p), step), step), :]

    def block_of(group, yy, core):
        return tokens.at[group, pl.ds(pl.multiple_of((2 * yy + core) * rows, rows), rows), :]

    def pass_on(way, group, yy, p):
        piece = piece_of(group, yy, p)
        height = lax.div(group, 2)
        if way == 2:
            receive = across_recv.at[height, yy]
        elif way == 3:
            receive = mate_recv.at[group, yy]
        else:
            receive = tok_recv.at[height, yy, p]
        return remote(piece, piece, tok_send.at[way], receive, devices[way])

    def sent(way, group_count, row_count):
        rows_sent = tokens.at[pl.ds(0, group_count), pl.ds(0, row_count), :]
        return remote(rows_sent, rows_sent, tok_send.at[way], mate_recv.at[0, 0], devices[way])

    def along_z(group, yy, p):
        for way in range(2):

            @pl.when(routes[way](group))
            def _():
                pass_on(way, group, yy, p).start()

    for p in range(PIECES):
        y_copy(p).wait_recv()
        piece = pl.ds(pl.multiple_of(offset_of(p), step), step)
        residual = (
            stream_ref[piece, :].astype(f32) + (pair_sum(y, p) + y_in[piece, :].astype(f32))
        ).astype(bf16)
        resid[piece, :] = residual
        tokens[sp, pl.ds(pl.multiple_of(tp * rows + offset_of(p), step), step), :] = scaled_norm(
            residual.astype(f32), gain_ref[...].reshape(1, width)
        ).astype(bf16)
        pass_on(4, sp, y, p).start()
        along_z(sp, y, p)
        pass_on(2, sp, y, p).start()
        pass_on(3, sp, y, p).start()

    loaded("gate", "up", "down")

    def wait_piece(group, yy, p):
        pass_on(0, group, yy, p).wait_recv()

    def wait_mate(group, yy):
        block = block_of(group, yy, 1 - c)
        remote(block, block, tok_send.at[3], mate_recv.at[group, yy], at(sp, sibling)).wait_recv()

    def block_at(code):
        relative, second, p = lax.div(code, 2 * PIECES), lax.rem(lax.div(code, PIECES), 2), lax.rem(code, PIECES)
        return relative, height_of(relative), jnp.where(second == 0, y, 1 - y), p

    def take(code):
        relative, height, yy, p = block_at(code)
        group = 2 * height + x

        @pl.when((relative > 0) & (lax.rem(code, 2 * PIECES) == 0))
        def _():
            wait_scales(group)
            send_scales(group)

        wait_piece(group, yy, p)

        @pl.when((relative > 0) | at_end)
        def _():
            along_z(group, yy, p)

        pass_on(3, group, yy, p).start()

        @pl.when(relative > 0)
        def _():
            pass_on(2, group, yy, p).start()

    def take_across(code):
        _, height, yy, _ = block_at(code)
        group = 2 * height + 1 - x

        @pl.when(lax.rem(code, 2 * PIECES) == 0)
        def _():
            wait_scales(group)

        block = block_of(group, yy, c)
        remote(block, block, tok_send.at[2], across_recv.at[height, yy], devices[2]).wait_recv()
        remote(block, block, tok_send.at[3], mate_recv.at[group, yy], devices[3]).start()

    def pass_held(code):
        p = lax.rem(code, PIECES)

        @pl.when(code < PIECES)
        def _():
            pass_on(2, sp, 1 - y, p).start()

        @pl.when(code >= PIECES)
        def _():
            along_z(sp, 1 - y, p)

    def tile_at(tile):
        height = height_of(lax.div(tile, 4))
        side = jnp.where(lax.rem(lax.div(tile, 2), 2) == 0, x, 1 - x)
        return height, 2 * height + side, jnp.where(lax.rem(tile, 2) == 0, y, 1 - y)

    def tile_rows(yy):
        return pl.ds(pl.multiple_of(yy * half, half), half)

    def share(way, group, yy):
        whose = tp if way < 2 else opposite
        block = hidden.at[group, whose, tile_rows(yy), :]
        receive = mate_hid_recv.at[group, yy] if way else hid_recv.at[group, yy]
        return remote(block, block, hid_send.at[way], receive, at(sp, sibling if way else opposite))

    def gated_units(tile):
        _, group, yy = tile_at(tile)
        wait_mate(group, yy)
        inputs = tokens[group, tile_rows(yy), :]
        span = min(256, units)
        for start in range(0, units, span):
            gate_pre = jnp.dot(inputs, gate_w[:, start : start + span], preferred_element_type=f32)
            up_pre = jnp.dot(inputs, up_w[:, start : start + span], preferred_element_type=f32)
            hidden[group, tp, tile_rows(yy), start : start + span] = clamped_units(gate_pre, up_pre).astype(bf16)
        share(0, group, yy).start()
        share(1, group, yy).start()

    def relay_units(tile):
        _, group, yy = tile_at(tile)
        share(0, group, yy).wait_recv()
        share(2, group, yy).start()

    def own_half(yy, h):
        return pl.ds(pl.multiple_of(yy * half + h * rows, rows), rows)

    def chain_copy(group, yy, h):
        rising = lax.div(group, 2) > z
        return remote(
            part.at[group, own_half(yy, h), :],
            chain_in.at[jnp.where(at_end, 0, 1), group, own_half(yy, h), :],
            chain_send.at[0],
            chain_recv.at[group, yy, h],
            at(sp + jnp.where(rising, 2, -2), tp),
        )

    def wait_chain(sides, group, yy, h):
        tiles = chain_in.at[pl.ds(0, sides), group, own_half(yy, h), :]
        remote(tiles, tiles, chain_send.at[0], chain_recv.at[group, yy, h], at(sp, sibling)).wait_recv()

    diagonal = lax.broadcasted_iota(jnp.int32, (half, half), 0) == lax.broadcasted_iota(jnp.int32, (half, half), 1)

    def project_down(tile):
        _, group, yy = tile_at(tile)
        both = hidden.at[group, pl.ds(0, 2), tile_rows(yy), :]
        remote(both, both, hid_send.at[1], mate_hid_recv.at[group, yy], at(sp, sibling)).wait_recv()
        own_rows = tile_rows(yy)
        out = jnp.dot(hidden[group, 0, own_rows, :], down_w[:units, :], preferred_element_type=f32)
        for k in range(1, 4):
            out = out + jnp.dot(
                hidden[group, k, own_rows, :], down_w[k * units : (k + 1) * units, :], preferred_element_type=f32
            )
        weight = scales[group, :, tile_rows(yy)]
        mine = lax.broadcasted_iota(jnp.int32, weight.shape, 0) == sp
        weight = jnp.sum(jnp.where(mine, weight, 0.0), axis=0, keepdims=True)
        weight = jnp.sum(jnp.where(diagonal, weight, 0.0), axis=1, keepdims=True)
        part[group, own_rows, :] = (out.astype(bf16).astype(f32) * weight).astype(bf16)

    def x_copy(group, yy, h):
        height = lax.div(group, 2)
        return remote(
            part.at[group, own_half(yy, h), :],
            x_in.at[height, own_half(yy, h), :],
            x_send.at[0],
            x_recv.at[height, yy, h],
            at(across, tp),
        )

    def hand_over(to):
        return remote(
            final.at[pl.ds(to * rows, rows), :], columns.at[tp], fin_send.at[0], fin_recv.at[tp], at(sp, to)
        )

    def flag(words, position):
        return lax.rem(lax.shift_right_logical(jnp.where(at_end, words[0], words[1]), position), 2)

    x_first_words = [sum(1 << (2 * height + second) for height, second in chosen) for chosen in x_first]
    near_words, far_words = comes_along_z(*x_first)

    def toward_home(code):
        tile, h = lax.div(code, 2), lax.rem(code, 2)
        relative, second = lax.div(tile, 4), lax.rem(tile, 2)
        height, group, yy = tile_at(tile)
        own_rows = own_half(yy, h)
        own_side = lax.rem(lax.div(tile, 2), 2) == 0
        over_x = (relative == 0) | (flag(x_first_words, 2 * relative + second) == 1)
        near, far = flag(near_words, tile), flag(far_words, tile)
        total[...] = part[group, own_rows, :].astype(f32)
        for count in (1, 2):

            @pl.when(near + far == count)
            def _():
                wait_chain(count, group, yy, h)

        for side, comes in enumerate((near, far)):

            @pl.when(comes == 1)
            def _():
                total[...] = total[...] + chain_in[side, group, own_rows, :].astype(f32)

        @pl.when(own_side & over_x)
        def _():
            x_copy(group, yy, h).wait_recv()
            total[...] = total[...] + x_in[height, own_rows, :].astype(f32)

        @pl.when(group != sp)
        def _():
            part[group, own_rows, :] = total[...].astype(bf16)

            @pl.when(own_side | jnp.logical_not(over_x))
            def _():
                chain_copy(group, yy, h).start()

            @pl.when(jnp.logical_not(own_side) & over_x)
            def _():
                x_copy(group, yy, h).start()

        @pl.when(group == sp)
        def _():
            final[own_rows, :] = total[...].astype(bf16)
            for to in range(4):

                @pl.when((tp != to) & (2 * yy + h == to))
                def _():
                    hand_over(to).start()

    acts = (take, take_across, pass_held, gated_units, relay_units, project_down, toward_home)

    def four_events(position, carry):
        word = pick(at_end, plans, position)

        def event(i, carry):
            code = lax.shift_right_logical(word, 8 * i) & 255
            kind, rest = lax.div(code, 32), lax.rem(code, 32)
            for j, act in enumerate(acts):

                @pl.when(kind == j)
                def _():
                    act(rest)

            return carry

        return lax.fori_loop(0, 4, event, carry)

    plans = [words_of(plan) for plan in (end_plan, middle_plan)]
    lax.fori_loop(0, max(len(plan) for plan in plans), four_events, 0)

    columns[tp] = final[pl.ds(pl.multiple_of(tp * rows, rows), rows), :]
    for by in (1, 2, 3):
        whose = lax.rem(tp + by, 4)
        remote(
            final.at[pl.ds(0, rows), :], columns.at[whose], fin_send.at[0], fin_recv.at[whose], at(sp, sibling)
        ).wait_recv()
    loaded("post_gain")
    combined = jnp.concatenate([columns[k] for k in range(4)], 1).astype(f32)
    result_ref[...] = (
        resid[...].astype(f32) + scaled_norm(combined, post_gain_ref[...].reshape(1, width))
    ).astype(bf16)

    @pl.when(sp < sp_count - 1)
    def _():
        rim_copy.wait_send()

    remote(pair_send, pair_in, pair_sem.at[0], pair_recv.at[0], at(sp, sibling)).wait_send()
    remote(y_send, y_in, y_sem.at[0], y_recv.at[0], at(sp, opposite)).wait_send()
    sent(4, 1, rows).wait_send()
    sent(3, heights, seq).wait_send()
    sent(2, heights, half).wait_send()

    def scales_sent(way, group_count):
        blocks = scales.at[pl.ds(0, group_count)]
        remote(blocks, blocks, scale_send.at[way], scale_recv.at[0], devices[way]).wait_send()

    scales_sent(2, heights)
    for count in range(1, heights):
        for way, its in enumerate((z == count - 1, z == heights - count)):

            @pl.when(its)
            def _():
                sent(way, count, half).wait_send()
                scales_sent(way, count)

    for way in range(3):
        tiles = hidden.at[:, 0]
        receive = mate_hid_recv.at[0, 0] if way else hid_recv.at[0, 0]
        remote(tiles, tiles, hid_send.at[way], receive, at(sp, sibling)).wait_send()
    for chosen, its in zip(x_first, (at_end, jnp.logical_not(at_end))):

        @pl.when(its)
        def _():
            crossed = part.at[pl.ds(0, len(chosen) + 2), pl.ds(0, half), :]
            remote(crossed, crossed, x_send.at[0], x_recv.at[0, 0, 0], at(across, tp)).wait_send()
            rising = 2 * (sp_count - 2) - len(chosen)
            across_count = 1 if rising <= sp_count else 2 if rising % 2 == 0 else 3
            chained = hidden.at[pl.ds(0, rising // across_count), pl.ds(0, across_count), pl.ds(0, half), :]
            remote(chained, chained, chain_send.at[0], chain_recv.at[0, 0, 0], at(sp, sibling)).wait_send()

    handed = final.at[pl.ds(0, 3 * rows), :]
    remote(handed, handed, fin_send.at[0], fin_recv.at[0], at(sp, sibling)).wait_send()


def dense_layer(
    stream_in,
    pre_gate,
    value_in,
    post_gate,
    conv_taps,
    out_weight,
    route_ids,
    route_weight,
    ffn_gain,
    post_gain,
    gate_proj,
    up_proj,
    down_proj,
):
    sp_count = lax.axis_size("sp")
    rows, width = stream_in.shape
    seq, channels = pre_gate.shape
    units = gate_proj.shape[2]
    cols = down_proj.shape[2]
    bf16, f32 = jnp.bfloat16, jnp.float32
    dma = pltpu.SemaphoreType.DMA
    small = (
        stream_in, pre_gate, value_in, post_gate, conv_taps, route_ids.T, route_weight.T, ffn_gain, post_gain
    )
    scratch = [pltpu.VMEM(array.shape, array.dtype) for array in small] + [
        pltpu.VMEM(out_weight.shape, bf16),
        pltpu.VMEM(gate_proj.shape[1:], bf16),
        pltpu.VMEM(up_proj.shape[1:], bf16),
        pltpu.VMEM(down_proj.shape[1:], bf16),
        pltpu.VMEM((16, channels), bf16),
        pltpu.VMEM((16, channels), bf16),
        pltpu.VMEM((seq + 8, channels), f32),
        pltpu.VMEM((seq, channels), bf16),
        pltpu.VMEM((2 * rows, width), bf16),
        pltpu.VMEM((2 * rows, width), bf16),
        pltpu.VMEM((2 * rows, width), f32),
        pltpu.VMEM((rows, width), bf16),
        pltpu.VMEM((rows, width), bf16),
        pltpu.VMEM((rows, width), bf16),
        pltpu.VMEM((sp_count, sp_count, seq), f32),
        pltpu.VMEM((sp_count, seq, width), bf16),
        pltpu.VMEM((sp_count, 4, seq, units), bf16),
        pltpu.VMEM((sp_count, seq, cols), bf16),
        pltpu.VMEM((2, sp_count, seq, cols), bf16),
        pltpu.VMEM((sp_count // 2, seq, cols), bf16),
        pltpu.VMEM((rows, cols), f32),
        pltpu.VMEM((seq, cols), bf16),
        pltpu.VMEM((4, rows, cols), bf16),
        dma((13,)),
        dma((2,)),
        dma((1,)),
        dma((4,)),
        dma((1,)),
        dma((PIECES,)),
        dma((3,)),
        dma((sp_count,)),
        dma((5,)),
        dma((sp_count // 2, 2, PIECES)),
        dma((sp_count // 2, 2)),
        dma((sp_count, 2)),
        dma((3,)),
        dma((sp_count, 2)),
        dma((sp_count, 2)),
        dma((1,)),
        dma((sp_count, 2, 2)),
        dma((1,)),
        dma((sp_count // 2, 2, 2)),
        dma((1,)),
        dma((4,)),
    ]
    vmem = pl.BlockSpec(memory_space=pltpu.VMEM)
    anywhere = pl.BlockSpec(memory_space=pl.ANY)
    return pl.pallas_call(
        functools.partial(layer_kernel, sp_count),
        out_shape=jax.ShapeDtypeStruct((rows, width), bf16),
        in_specs=[anywhere] * 13,
        out_specs=vmem,
        scratch_shapes=scratch,
        compiler_params=pltpu.CompilerParams(
            collective_id=0, has_side_effects=True, vmem_limit_bytes=58 * 1024 * 1024
        ),
    )(
        *small,
        out_weight,
        gate_proj,
        up_proj,
        down_proj,
    )


def local(
    stream_in,
    pre_gate,
    value_in,
    post_gate,
    conv_taps,
    out_weight,
    route_ids,
    route_weight,
    ffn_gain,
    post_gain,
    gate_proj,
    up_proj,
    down_proj,
):
    sp_count = lax.axis_size("sp")
    tp_count = lax.axis_size("tp")
    seq_rows = pre_gate.shape[0]
    own_rows = seq_rows // tp_count
    top_count = route_ids.shape[1]
    slots_each = 2 * own_rows * top_count // sp_count
    if tp_count == 4 and sp_count == PLANNED_GROUPS and slots_each >= own_rows:
        return dense_layer(
            stream_in, pre_gate, value_in, post_gate, conv_taps, out_weight, route_ids, route_weight,
            ffn_gain, post_gain, gate_proj, up_proj, down_proj,
        )
    tap_count = conv_taps.shape[0]
    gated_input = (pre_gate.astype(jnp.float32) * value_in.astype(jnp.float32)).astype(jnp.bfloat16)
    rim_rows = passed_along(gated_input[seq_rows - tap_count + 1 :], "sp", 1)
    padded = jnp.concatenate([rim_rows, gated_input], 0).astype(jnp.float32)
    convolved = jnp.zeros(gated_input.shape, jnp.float32)
    for tap_index in range(tap_count):
        convolved = (
            convolved
            + conv_taps[tap_index].astype(jnp.float32)[None, :]
            * padded[tap_index : tap_index + seq_rows]
        )
    mixer_out = (post_gate.astype(jnp.float32) * convolved).astype(jnp.bfloat16)
    weight_rows = mixer_out
    projected = lax.psum_scatter(
        jnp.dot(weight_rows, out_weight, preferred_element_type=jnp.float32),
        "tp",
        scatter_dimension=0,
        tiled=True,
    )
    residual = (stream_in.astype(jnp.float32) + projected).astype(jnp.bfloat16)
    normed = scaled_norm(residual.astype(jnp.float32), ffn_gain).astype(jnp.bfloat16)
    slot_rank = block_ranks(route_ids, sp_count, own_rows)
    block_of = (jnp.arange(seq_rows, dtype=jnp.int32) // own_rows)[:, None]
    tp_index = lax.axis_index("tp")
    own_ids = lax.dynamic_slice_in_dim(route_ids, tp_index * own_rows, own_rows, 0)
    own_rank = lax.dynamic_slice_in_dim(slot_rank, tp_index * own_rows, own_rows, 0)
    own_slot = own_ids * slots_each + own_rank
    picker = slot_picker(own_slot, sp_count * slots_each)
    outgoing = jnp.dot(picker, normed, preferred_element_type=jnp.float32).astype(jnp.bfloat16)
    arrived = lax.all_to_all(outgoing, "sp", split_axis=0, concat_axis=0, tiled=True)
    portion = lax.all_gather(arrived, "tp", axis=0, tiled=True)
    gate_pre = jnp.dot(portion, gate_proj[0], preferred_element_type=jnp.float32)
    up_pre = jnp.dot(portion, up_proj[0], preferred_element_type=jnp.float32)
    hidden = clamped_units(gate_pre, up_pre).astype(jnp.bfloat16)
    weight_rows = down_proj[0]
    column_out = jnp.dot(
        lax.all_gather(hidden, "tp", axis=1, tiled=True),
        weight_rows,
        preferred_element_type=jnp.float32,
    ).astype(jnp.bfloat16)
    column_width = column_out.shape[1]
    returned = lax.all_to_all(
        column_out.reshape(tp_count, sp_count, slots_each, column_width),
        "sp",
        split_axis=1,
        concat_axis=1,
        tiled=True,
    )
    home_index = (block_of * sp_count + route_ids) * slots_each + slot_rank
    gathered_out = jnp.take(returned.reshape(-1, column_width), home_index.reshape(-1), axis=0)
    gathered_out = gathered_out.astype(jnp.float32).reshape(seq_rows, top_count, column_width)
    combined_cols = jnp.sum(gathered_out * route_weight[:, :, None], axis=1).astype(jnp.bfloat16)
    combined = lax.all_to_all(combined_cols, "tp", split_axis=0, concat_axis=1, tiled=True)
    layer_out = residual.astype(jnp.float32) + scaled_norm(combined.astype(jnp.float32), post_gain)
    return layer_out.astype(jnp.bfloat16)


def solution(mesh):
    placed = (
        P(("sp", "tp"), None),
        P("sp", "tp"),
        P("sp", "tp"),
        P("sp", "tp"),
        P(None, "tp"),
        P("tp", None),
        P("sp", None),
        P("sp", None),
        P(),
        P(),
        P("sp", None, "tp"),
        P("sp", None, "tp"),
        P("sp", None, "tp"),
    )
    return jax.shard_map(
        local, mesh=mesh, in_specs=placed, out_specs=P(("sp", "tp"), None), check_vma=False
    )
```
